128 devices in a mesh: rep: 2 (over z_hi), fs: 32 (over z_lo, y, x), tp: 2 (over core).
Axes of the slice: x: 4, y: 4, z: 4 (z_hi: 2, z_lo: 2; z = z_hi * 2 + z_lo), core: 2. Of those that a mesh axis runs over, the one named last changes fastest.
Arguments:
- tokens: bfloat16 [49152, 2048], P(('rep', 'fs', 'tp')), may hold values from -6 to 6
- outer_weight: float32 [2048, 1536], P('fs', 'tp'), may hold values from -0.125 to 0.125
- inner_weight: float32 [2048, 1536], P('fs', 'tp'), may hold values from -0.125 to 0.125
- value_weight: float32 [2048, 1536], P('fs', 'tp'), may hold values from -0.125 to 0.125
- conv_taps: float32 [3, 1536], P(None, 'tp'), may hold values from -3 to 3
- mix_out: float32 [1536, 2048], P('tp', 'fs'), may hold values from -0.15625 to 0.15625
- norm_first: float32 [2048], replicated, may hold values from 0.1 to 1.9
- up_weight: float32 [2048, 4096], P('fs', 'tp'), may hold values from -0.125 to 0.125
- down_weight: float32 [4096, 2048], P('tp', 'fs'), may hold values from -0.09375 to 0.09375
- norm_second: float32 [2048], replicated, may hold values from 0.1 to 1.9
Outputs:
- encoded: bfloat16 [49152, 2048], P(('rep', 'fs', 'tp'))
The draws below stay inside these ranges and needn't reach their ends.
All inputs are finite; a program needn't handle non-finite values.
Results may differ from the reference program's by a relative error of at most 0.015.
Values may be sent and summed in bfloat16 or wider, within the bound.
No kernel may reach another device: no remote copies, remote signals or barrier semaphores. Data moves between devices by JAX's collectives and lax.ppermute only.
A program may use at most 128 MiB of HBM per device.

```python
import jax
import jax.numpy as jnp
from jax import lax

D = 2048
WA = 1536
FF = 4096
SEQ = 128
TOK_DEV = 384
TOKENS = 49152


def level_of(own_key, dims, split, least, top_value):
    gain, own = 1.0, jax.random.fold_in(own_key, 6)
    for axis_at, parts in split:
        steps = jnp.exp(jax.random.uniform(jax.random.fold_in(own, axis_at), (parts,), jnp.float32, least / len(split), top_value / len(split)))
        gain = gain * jnp.repeat(steps, dims[axis_at] // parts).reshape([-1 if axis == axis_at else 1 for axis in range(len(dims))])
    return gain


def gaussian(rng, dims, width, reach, split=(), kind=jnp.bfloat16):
    drawn = jax.random.normal(rng, dims, jnp.float32) * width
    if len(split) > 0:
        drawn = level_of(rng, dims, split, -0.22, 0.18) * drawn
    return jnp.clip(drawn, min=-reach, max=reach).astype(kind)


def setup_inputs(seed: int = 0) -> dict:
    arg_keys = jax.random.split(jax.random.key(seed), 11)
    tokens = gaussian(arg_keys[0], (TOKENS, D), 1.0, 6.0, ((0, 128),))
    outer_weight = gaussian(arg_keys[1], (D, WA), D ** -0.5, 0.125, ((0, 32), (1, 2)), jnp.float32)
    inner_weight = gaussian(arg_keys[2], (D, WA), D ** -0.5, 0.125, ((0, 32), (1, 2)), jnp.float32)
    value_weight = gaussian(arg_keys[3], (D, WA), D ** -0.5, 0.125, ((0, 32), (1, 2)), jnp.float32)
    conv_taps = gaussian(arg_keys[4], (3, WA), 0.6, 3.0, ((1, 2),), jnp.float32)
    mix_out = gaussian(arg_keys[5], (WA, D), WA ** -0.5, 0.15625, ((0, 2), (1, 32)), jnp.float32)
    norm_first = jnp.clip(1.0 + 0.18 * jax.random.normal(arg_keys[6], (D,), jnp.float32), 0.1, 1.9)
    up_weight = gaussian(arg_keys[7], (D, FF), D ** -0.5, 0.125, ((0, 32), (1, 2)), jnp.float32)
    down_weight = gaussian(arg_keys[8], (FF, D), FF ** -0.5, 0.09375, ((0, 2), (1, 32)), jnp.float32)
    norm_second = jnp.clip(1.0 + 0.18 * jax.random.normal(arg_keys[9], (D,), jnp.float32), 0.1, 1.9)
    return {"tokens": tokens, "outer_weight": outer_weight, "inner_weight": inner_weight, "value_weight": value_weight, "conv_taps": conv_taps, "mix_out": mix_out, "norm_first": norm_first, "up_weight": up_weight, "down_weight": down_weight, "norm_second": norm_second}


residual_scale = 2.0 ** 0.25
norm_epsilon = 1e-05

def layer_norm(values, scaling):
    center = values - lax.optimization_barrier(jnp.mean(values, axis=-1, keepdims=True))
    spread = lax.optimization_barrier(jnp.mean(center * center, axis=-1, keepdims=True))
    return center * lax.rsqrt(spread + norm_epsilon) * scaling

def reference(tokens, outer_weight, inner_weight, value_weight, conv_taps, mix_out, norm_first, up_weight, down_weight, norm_second):
    outer_bf = outer_weight.astype(jnp.bfloat16)
    inner_bf = inner_weight.astype(jnp.bfloat16)
    value_bf = value_weight.astype(jnp.bfloat16)
    mixout_bf = mix_out.astype(jnp.bfloat16)
    upward_bf = up_weight.astype(jnp.bfloat16)
    downward_bf = down_weight.astype(jnp.bfloat16)
    blocks = tokens.reshape(-1, TOK_DEV * 8, D)

    def one_block(rows):
        outer = jnp.dot(rows, outer_bf, preferred_element_type=jnp.float32)
        inner = jnp.dot(rows, inner_bf, preferred_element_type=jnp.float32)
        value = jnp.dot(rows, value_bf, preferred_element_type=jnp.float32)
        framed = (inner * value).reshape(-1, SEQ, WA)
        padded = jnp.pad(framed, ((0, 0), (1, 1), (0, 0)))
        convolved = padded[:, :-2] * conv_taps[0] + framed * conv_taps[1] + padded[:, 2:] * conv_taps[2]
        mixed = (outer * convolved.reshape(-1, WA)).astype(jnp.bfloat16)
        mixing = jnp.dot(mixed, mixout_bf, preferred_element_type=jnp.float32)
        first = layer_norm(residual_scale * rows.astype(jnp.float32) + mixing, norm_first).astype(jnp.bfloat16)
        raised = jax.nn.relu(jnp.dot(first, upward_bf, preferred_element_type=jnp.float32))
        hidden = (raised * raised).astype(jnp.bfloat16)
        lowered = jnp.dot(hidden, downward_bf, preferred_element_type=jnp.float32)
        return layer_norm(residual_scale * first.astype(jnp.float32) + lowered, norm_second).astype(jnp.bfloat16)
    return lax.map(one_block, blocks).reshape(tokens.shape[0], D)
```

```python
import jax
import jax.numpy as jnp
from jax import lax
from jax.sharding import Mesh
from jax.sharding import PartitionSpec as P

SEQ = 128
FS = ("fs_0", "fs_1", "fs_2")
REP_FS = ("rep", "fs_0", "fs_1", "fs_2")
REP_FS_TP = ("rep", "fs_0", "fs_1", "fs_2", "tp")


residual_scale = 2.0**0.25
norm_epsilon = 1e-05


def own_half(x, dim):
    length = x.shape[dim] // 2
    return lax.dynamic_slice_in_dim(x, lax.axis_index("rep") * length, length, dim)


def gathered_halves(x):
    full = lax.all_gather(x, REP_FS, axis=0, tiled=True)
    return full.reshape(2, -1, x.shape[1])


def sum_at_owner(x, axis):
    tiles = x.reshape(2, -1, x.shape[1])
    arrived = lax.all_to_all(tiles, axis, split_axis=0, concat_axis=0, tiled=True)
    return arrived.astype(jnp.float32).sum(axis=0)


def layer_norm(values, scaling):
    center = values - jnp.mean(values, axis=-1, keepdims=True)
    spread = jnp.mean(center * center, axis=-1, keepdims=True)
    return center * lax.rsqrt(spread + norm_epsilon) * scaling


def short_conv(product, conv_taps):
    places = jnp.arange(product.shape[0], dtype=jnp.int32) % SEQ
    blank = jnp.zeros((1, product.shape[1]), jnp.float32)
    before = jnp.concatenate([blank, product[:-1]], axis=0)
    after = jnp.concatenate([product[1:], blank], axis=0)
    before = jnp.where((places > 0)[:, None], before, 0.0)
    after = jnp.where((places < SEQ - 1)[:, None], after, 0.0)
    return conv_taps[0] * before + conv_taps[1] * product + conv_taps[2] * after


def dot(a, b):
    return jnp.dot(a, b, preferred_element_type=jnp.float32)


def dot_t(a, b):
    return lax.dot_general(a, b, (((1,), (1,)), ((), ())), preferred_element_type=jnp.float32)


def local(
    tokens,
    outer_weight,
    inner_weight,
    value_weight,
    conv_taps,
    mix_out,
    norm_first,
    up_weight,
    down_weight,
    norm_second,
):
    bf = jnp.bfloat16
    grouped = lax.all_gather(tokens, "tp", axis=0, tiled=True)
    into = jnp.concatenate(
        [own_half(w, 1).astype(bf) for w in (outer_weight, inner_weight, value_weight)], axis=1
    )
    into_full = gathered_halves(into)
    mixout_full = gathered_halves(own_half(mix_out, 0).astype(bf).T)
    up_full = gathered_halves(own_half(up_weight, 1).astype(bf))
    down_full = gathered_halves(own_half(down_weight, 0).astype(bf).T)

    width = into.shape[1] // 3
    mixing = 0.0
    for h in range(2):
        w = into_full[h]
        outer = dot(grouped, w[:, :width])
        inner = dot(grouped, w[:, width : 2 * width])
        value = dot(grouped, w[:, 2 * width :])
        taps = conv_taps[:, h * width : (h + 1) * width]
        mixed = (outer * short_conv(inner * value, taps)).astype(bf)
        mixing = mixing + dot_t(mixed, mixout_full[h])
    mixing = sum_at_owner(mixing.astype(bf), "tp")
    first = layer_norm(residual_scale * tokens.astype(jnp.float32) + mixing, norm_first).astype(bf)
    grouped_first = lax.all_gather(first, "tp", axis=0, tiled=True)
    lowered = 0.0
    for h in range(2):
        raised = jax.nn.relu(dot(grouped_first, up_full[h]))
        hidden = (raised * raised).astype(bf)
        lowered = lowered + dot_t(hidden, down_full[h])
    lowered = sum_at_owner(lowered.astype(bf), "tp")
    return layer_norm(residual_scale * first.astype(jnp.float32) + lowered, norm_second).astype(bf)


def solution(mesh):
    finer = Mesh(
        mesh.devices.reshape(mesh.shape["rep"], 2, 4, 4, mesh.shape["tp"]),
        ("rep", "fs_0", "fs_1", "fs_2", "tp"),
    )
    placed = (
        P(REP_FS_TP, None),
        P(FS, "tp"),
        P(FS, "tp"),
        P(FS, "tp"),
        P(None, "tp"),
        P("tp", FS),
        P(),
        P(FS, "tp"),
        P("tp", FS),
        P(),
    )
    return jax.shard_map(
        local, mesh=finer, in_specs=placed, out_specs=P(REP_FS_TP, None), check_vma=False
    )
```

```python
import functools

import jax
import jax.numpy as jnp
from jax import lax
from jax.experimental import pallas as pl
from jax.experimental.pallas import tpu as pltpu
from jax.sharding import Mesh
from jax.sharding import PartitionSpec as P

SEQ = 128
D = 2048
ROWS = 32
FS = ("fs_0", "fs_1", "fs_2")
REP_FS_TP = ("rep", "fs_0", "fs_1", "fs_2", "tp")
CHIPS = (4, 4, 4)
ORDERS = ("zxy", "xyz", "yzx")
CHANNELS = 256
HIDDEN = ((384, 384, 256), (384, 256, 384))


residual_scale = 2.0**0.25
norm_epsilon = 1e-05
bf = jnp.bfloat16
ANY = pl.BlockSpec(memory_space=pl.ANY)
VMEM = pl.BlockSpec(memory_space=pltpu.VMEM)
PARAMS = pltpu.CompilerParams(vmem_limit_bytes=48 * 1024 * 1024)


def hidden_start(stage, part):
    return sum(HIDDEN[0]) * stage + sum(HIDDEN[stage][:part])


def stage_widths(part):
    return [4 * CHANNELS] + [2 * HIDDEN[s][part] for s in range(2)]


def position(axis):
    if axis == "z":
        return lax.axis_index("rep") * 2 + lax.axis_index("fs_0")
    return lax.axis_index({"y": "fs_1", "x": "fs_2"}[axis])


def source(axis, step):
    way = 2 * lax.axis_index("tp") - 1
    return (position(axis) + 4 + way * step) & 3


def ring_pairs(axis):
    at = "zyx".index(axis)
    pairs = []
    for z in range(4):
        for y in range(4):
            for x in range(4):
                for core in range(2):
                    to = [z, y, x]
                    to[at] = (to[at] + (1 if core == 0 else 3)) % 4
                    start = ((z * 4 + y) * 4 + x) * 2 + core
                    pairs.append((start, ((to[0] * 4 + to[1]) * 4 + to[2]) * 2 + core))
    return pairs


def around(block, axis):
    blocks = [block]
    for _ in range(3):
        blocks.append(lax.ppermute(blocks[-1], REP_FS_TP, ring_pairs(axis)))
    return blocks


def swapped(x):
    return lax.ppermute(x, "tp", [(0, 1), (1, 0)])


def finish(copies):
    for copy in copies:
        copy.start()
    for copy in copies:
        copy.wait()


def pieces_kernel(outer, inner, value, mix, up, down, *refs):
    outs, mix_t, down_t = refs[:3], refs[3], refs[4]
    mix_t[...] = mix[...].T
    down_t[...] = down[...].T
    rows = pl.ds(lax.axis_index("rep") * ROWS, ROWS)
    for part, out in enumerate(outs):
        at = 0
        for w in (outer, inner, value, mix_t):
            out[:, at : at + CHANNELS] = w[rows, part * CHANNELS : (part + 1) * CHANNELS].astype(bf)
            at += CHANNELS
        for s in range(2):
            start, n = hidden_start(s, part), HIDDEN[s][part]
            for w in (up, down_t):
                out[:, at : at + n] = w[rows, start : start + n].astype(bf)
                at += n


def pieces(*weights):
    return pl.pallas_call(
        pieces_kernel,
        out_shape=[jax.ShapeDtypeStruct((ROWS, sum(stage_widths(c))), bf) for c in range(3)],
        in_specs=[VMEM] * 6,
        out_specs=[VMEM] * 3,
        scratch_shapes=[pltpu.VMEM((64, 3 * CHANNELS), jnp.float32), pltpu.VMEM((64, D), jnp.float32)],
        compiler_params=PARAMS,
    )(*weights)


def place_kernel(axis, widths, *refs):
    parts, outs, sems = refs[:4], refs[4:-1], refs[-1]
    copies = []
    for k, part in enumerate(parts):
        at = 0
        for i, width in enumerate(widths):
            copies.append(
                pltpu.make_async_copy(
                    part.at[..., pl.ds(at, width)],
                    outs[i].at[source(axis, k)],
                    sems.at[len(copies)],
                )
            )
            at += width
    finish(copies)


def placed(parts, axis, widths):
    lead = parts[0].shape[:-1]
    return pl.pallas_call(
        functools.partial(place_kernel, axis, widths),
        out_shape=[jax.ShapeDtypeStruct((4, *lead, w), bf) for w in widths],
        in_specs=[ANY] * 4,
        out_specs=[ANY] * len(widths),
        scratch_shapes=[pltpu.SemaphoreType.DMA((4 * len(widths),))],
        compiler_params=PARAMS,
    )(*parts)


def fill(order, blocks, start, width, whole, at, sems, used):
    copies = []

    def add(src, dst):
        copies.append(pltpu.make_async_copy(src, dst, sems.at[used + len(copies)]))

    cs, cd = pl.ds(start, width), pl.ds(at, width)
    for k, block in enumerate(blocks):
        p = source(order[2], k)
        if order == "xyz":
            add(block.at[:, :, :, cs], whole.at[p & 1, :, :, p >> 1, :, cd])
        else:
            for z in range(4):
                if order == "zxy":
                    add(block.at[:, z, :, cs], whole.at[z & 1, p, :, z >> 1, :, cd])
                else:
                    add(block.at[z, :, :, cs], whole.at[z & 1, :, p, z >> 1, :, cd])
    return copies


def whole_scratch(width):
    return pltpu.VMEM((2, 4, 4, 2, ROWS, width), bf)


def dot(a, b):
    return jnp.dot(a, b, preferred_element_type=jnp.float32)


def dot_t(a, b):
    return lax.dot_general(a, b, (((1,), (1,)), ((), ())), preferred_element_type=jnp.float32)


def both_tokens(own, other, x, sems, used):
    half = own.shape[0]
    return [
        pltpu.make_async_copy(own, x.at[pl.ds(0, half)], sems.at[used]),
        pltpu.make_async_copy(other, x.at[pl.ds(half, half)], sems.at[used + 1]),
    ]


def mixer_kernel(order, own, other, taps, *refs):
    blocks, mixed, x, w, sems = refs[:4], refs[4], refs[5], refs[6], refs[7]
    copies = both_tokens(own, other, x, sems, 0)
    copies += fill(order, blocks, 0, 3 * CHANNELS, w, 0, sems, 2)
    finish(copies)

    def product(i):
        return dot(x[...], w[..., i * CHANNELS : (i + 1) * CHANNELS].reshape(D, CHANNELS))

    gated = product(1) * product(2)
    place = lax.broadcasted_iota(jnp.int32, gated.shape, 0) & (SEQ - 1)
    before = jnp.where(place > 0, pltpu.roll(gated, 1, 0), 0.0)
    after = jnp.where(place < SEQ - 1, pltpu.roll(gated, gated.shape[0] - 1, 0), 0.0)
    conv = taps[0:1] * before + taps[1:2] * gated + taps[2:3] * after
    mixed[...] = (product(0) * conv).astype(bf)


def mixer(order, own, other, taps, blocks):
    rows = 2 * own.shape[0]
    return pl.pallas_call(
        functools.partial(mixer_kernel, order),
        out_shape=jax.ShapeDtypeStruct((rows, CHANNELS), bf),
        in_specs=[ANY, ANY, VMEM] + [ANY] * 4,
        out_specs=VMEM,
        scratch_shapes=[
            pltpu.VMEM((rows, D), bf),
            whole_scratch(3 * CHANNELS),
            pltpu.SemaphoreType.DMA((18,)),
        ],
        compiler_params=PARAMS,
        cost_estimate=pl.CostEstimate(
            flops=2 * rows * D * 3 * CHANNELS, bytes_accessed=8_000_000, transcendentals=0
        ),
    )(own, other, taps, *blocks)


def projected(left, whole, own, other, more=None):
    half = own.shape[0]

    def step(j, _):
        rows = whole[j >> 2, j & 3].reshape(256, whole.shape[-1])
        cols = pl.ds(pl.multiple_of(j * 256, 256), 256)
        sums = dot_t(left[...], rows)
        if more is not None:
            sums = sums + more[:, cols]
        own[:, cols] = sums[:half].astype(own.dtype)
        other[:, cols] = sums[half:].astype(other.dtype)
        return 0

    lax.fori_loop(0, 8, step, 0)


def mix_out_kernel(*refs):
    mixed, blocks = refs[:3], refs[3:15]
    own, other, left, whole, sems = refs[15:]
    copies = []
    for c, order in enumerate(ORDERS):
        at = c * CHANNELS
        part = blocks[4 * c : 4 * c + 4]
        copies += fill(order, part, 3 * CHANNELS, CHANNELS, whole, at, sems, len(copies))
        left[:, at : at + CHANNELS] = mixed[c][...]
    finish(copies)
    projected(left, whole, own, other)


def mix_out_product(mixed, blocks):
    rows = mixed[0].shape[0]
    return pl.pallas_call(
        mix_out_kernel,
        out_shape=[
            jax.ShapeDtypeStruct((rows // 2, D), jnp.float32),
            jax.ShapeDtypeStruct((rows // 2, D), bf),
        ],
        in_specs=[VMEM] * 3 + [ANY] * 12,
        out_specs=[VMEM] * 2,
        scratch_shapes=[
            pltpu.VMEM((rows, 3 * CHANNELS), bf),
            whole_scratch(3 * CHANNELS),
            pltpu.SemaphoreType.DMA((36,)),
        ],
        compiler_params=PARAMS,
        cost_estimate=pl.CostEstimate(
            flops=2 * rows * D * 3 * CHANNELS, bytes_accessed=9_000_000, transcendentals=0
        ),
    )(*mixed, *blocks)


def feed_kernel(stage, first_own, first_other, *refs):
    blocks, refs = refs[:12], refs[12:]
    more = None
    if stage == 1:
        more, refs = refs[0], refs[1:]
    if stage == 0:
        sums, x, up, down, hidden, sems = refs
    else:
        own, other, x, up, down, hidden, sems = refs
    copies = both_tokens(first_own, first_other, x, sems, 0)
    later = []
    for c, order in enumerate(ORDERS):
        n = HIDDEN[stage][c]
        at = sum(HIDDEN[stage][:c])
        part = blocks[4 * c : 4 * c + 4]
        copies += fill(order, part, 0, n, up, at, sems, len(copies))
    for c, order in enumerate(ORDERS):
        n = HIDDEN[stage][c]
        at = sum(HIDDEN[stage][:c])
        part = blocks[4 * c : 4 * c + 4]
        later += fill(order, part, n, n, down, at, sems, len(copies) + len(later))
    for copy in copies + later:
        copy.start()
    for copy in copies:
        copy.wait()

    for j in range(4):
        cols = slice(j * 256, (j + 1) * 256)
        raised = jnp.maximum(dot(x[...], up[..., cols].reshape(D, 256)), 0.0)
        hidden[:, cols] = (raised * raised).astype(bf)
    for copy in later:
        copy.wait()
    if stage == 0:
        half = sums.shape[0] // 2
        projected(hidden, down, sums.at[pl.ds(0, half)], sums.at[pl.ds(half, half)])
    else:
        projected(hidden, down, own, other, more)


def feed(stage, own, other, blocks, more=None):
    rows = 2 * own.shape[0]
    width = sum(HIDDEN[stage])
    if stage == 0:
        shapes = [jax.ShapeDtypeStruct((rows, D), jnp.float32)]
    else:
        shapes = [
            jax.ShapeDtypeStruct((rows // 2, D), jnp.float32),
            jax.ShapeDtypeStruct((rows // 2, D), bf),
        ]
    extra = [] if more is None else [more]
    return pl.pallas_call(
        functools.partial(feed_kernel, stage),
        out_shape=shapes,
        in_specs=[ANY] * 14 + [VMEM] * len(extra),
        out_specs=[VMEM] * len(shapes),
        scratch_shapes=[
            pltpu.VMEM((rows, D), bf),
            whole_scratch(width),
            whole_scratch(width),
            pltpu.VMEM((rows, width), bf),
            pltpu.SemaphoreType.DMA((80,)),
        ],
        compiler_params=PARAMS,
        cost_estimate=pl.CostEstimate(
            flops=4 * rows * D * width, bytes_accessed=20_000_000, transcendentals=0
        ),
    )(own, other, *blocks, *extra)


def layer_norm(values, scaling):
    center = values - jnp.mean(values, axis=-1, keepdims=True)
    spread = jnp.mean(center * center, axis=-1, keepdims=True)
    return center * lax.rsqrt(spread + norm_epsilon) * scaling


def joined(skip, own, other, scaling):
    sums = own + swapped(other).astype(jnp.float32)
    return layer_norm(residual_scale * skip.astype(jnp.float32) + sums, scaling).astype(bf)


def local(
    tokens,
    outer_weight,
    inner_weight,
    value_weight,
    conv_taps,
    mix_out,
    norm_first,
    up_weight,
    down_weight,
    norm_second,
):
    parts = pieces(outer_weight, inner_weight, value_weight, mix_out, up_weight, down_weight)
    tokens_other = swapped(tokens)
    near = [
        placed(around(part, order[0]), order[0], [part.shape[-1]])[0]
        for part, order in zip(parts, ORDERS)
    ]
    far = [
        placed(around(part, order[1]), order[1], stage_widths(c))
        for c, (part, order) in enumerate(zip(near, ORDERS))
    ]
    blocks = [[around(far[c][s], ORDERS[c][2]) for c in range(3)] for s in range(3)]

    mixed = [
        mixer(
            ORDERS[c],
            tokens,
            tokens_other,
            conv_taps[:, c * CHANNELS : (c + 1) * CHANNELS],
            blocks[0][c],
        )
        for c in range(3)
    ]
    flat = [sum(b, []) for b in blocks]
    own, other = mix_out_product(mixed, flat[0])
    first = joined(tokens, own, other, norm_first)
    first_other = swapped(first)
    (sums,) = feed(0, first, first_other, flat[1])
    own, other = feed(1, first, first_other, flat[2], sums)
    return joined(first, own, other, norm_second)


def solution(mesh):
    finer = Mesh(
        mesh.devices.reshape(2, 2, 4, 4, 2),
        ("rep", "fs_0", "fs_1", "fs_2", "tp"),
    )
    placement = (
        P(REP_FS_TP, None),
        P(FS, "tp"),
        P(FS, "tp"),
        P(FS, "tp"),
        P(None, "tp"),
        P("tp", FS),
        P(),
        P(FS, "tp"),
        P("tp", FS),
        P(),
    )
    return jax.shard_map(
        local, mesh=finer, in_specs=placement, out_specs=P(REP_FS_TP, None), check_vma=False
    )
```

```python
import functools

import jax
import jax.numpy as jnp
from jax import lax
from jax.experimental import pallas as pl
from jax.experimental.pallas import tpu as pltpu
from jax.sharding import Mesh
from jax.sharding import PartitionSpec as P


SEQ = 128
D = 2048
ROWS = 32
FS = ("fs_0", "fs_1", "fs_2")
REP_FS_TP = ("rep", "fs_0", "fs_1", "fs_2", "tp")
ORDERS = ("zxy", "xyz", "yzx")
CHANNELS = 256
HIDDEN = (768, 640, 640)


residual_scale = 2.0**0.25
norm_epsilon = 1e-05
bf = jnp.bfloat16
HBM = pl.BlockSpec(memory_space=pltpu.HBM)
VMEM = pl.BlockSpec(memory_space=pltpu.VMEM)
PARAMS = pltpu.CompilerParams(vmem_limit_bytes=48 * 1024 * 1024)


def in_hbm(arrays):
    return [pltpu.with_memory_space_constraint(a, pltpu.HBM) for a in arrays]


def stage_widths(part):
    return [4 * CHANNELS, 2 * HIDDEN[part]]


def position(axis):
    if axis == "z":
        return lax.axis_index("rep") * 2 + lax.axis_index("fs_0")
    return lax.axis_index({"y": "fs_1", "x": "fs_2"}[axis])


def source(axis, step):
    way = 2 * lax.axis_index("tp") - 1
    return (position(axis) + 4 + way * step) & 3


def ring_pairs(axis, step):
    at = "zyx".index(axis)
    pairs = []
    for z in range(4):
        for y in range(4):
            for x in range(4):
                for core in range(2):
                    to = [z, y, x]
                    to[at] = (to[at] + (step if core == 0 else 4 - step)) % 4
                    start = ((z * 4 + y) * 4 + x) * 2 + core
                    pairs.append((start, ((to[0] * 4 + to[1]) * 4 + to[2]) * 2 + core))
    return pairs


def moved(block, axis, step):
    return lax.ppermute(block, REP_FS_TP, ring_pairs(axis, step))


def around(block, axis):
    near, back = moved(block, axis, 1), moved(block, axis, 3)
    return [block, near, moved(near, axis, 1), back]


def swapped(x):
    return lax.ppermute(x, "tp", [(0, 1), (1, 0)])


def finish(copies):
    for copy in copies:
        copy.start()
    for copy in copies:
        copy.wait()


def pieces_kernel(*refs):
    weights, outs, held, sems = refs[:6], refs[6:9], refs[9:15], refs[15]
    rows = pl.ds(lax.axis_index("rep") * ROWS, ROWS)
    finish(
        [
            pltpu.make_async_copy(w.at[rows], h, sems.at[i])
            for i, (w, h) in enumerate(zip(weights, held))
        ]
    )
    outer, inner, value, mix, up, down = held
    for part, out in enumerate(outs):
        at = 0
        for w in (outer, inner, value, mix):
            out[:, at : at + CHANNELS] = w[:, part * CHANNELS : (part + 1) * CHANNELS].astype(bf)
            at += CHANNELS
        start, n = sum(HIDDEN[:part]), HIDDEN[part]
        for w in (up, down):
            out[:, at : at + n] = w[:, start : start + n].astype(bf)
            at += n


def pieces(*weights):
    return pl.pallas_call(
        pieces_kernel,
        out_shape=[jax.ShapeDtypeStruct((ROWS, sum(stage_widths(c))), bf) for c in range(3)],
        in_specs=[HBM] * 6,
        out_specs=[VMEM] * 3,
        scratch_shapes=[pltpu.VMEM((ROWS, w.shape[1]), jnp.float32) for w in weights]
        + [pltpu.SemaphoreType.DMA((6,))],
        compiler_params=PARAMS,
    )(*in_hbm(weights))


def place_kernel(axis, widths, *refs):
    parts, outs, sems = refs[:4], refs[4:-1], refs[-1]
    copies = []
    for k, part in enumerate(parts):
        at = 0
        for i, width in enumerate(widths):
            copies.append(
                pltpu.make_async_copy(
                    part.at[..., pl.ds(at, width)],
                    outs[i].at[source(axis, k)],
                    sems.at[len(copies)],
                )
            )
            at += width
    finish(copies)


def placed(parts, axis, widths):
    lead = parts[0].shape[:-1]
    return pl.pallas_call(
        functools.partial(place_kernel, axis, widths),
        out_shape=[pltpu.HBM((4, *lead, w), bf) for w in widths],
        in_specs=[HBM] * 4,
        out_specs=[HBM] * len(widths),
        scratch_shapes=[pltpu.SemaphoreType.DMA((4 * len(widths),))],
        compiler_params=PARAMS,
    )(*parts)


def fill(order, blocks, start, width, whole, at, sems, used):
    copies = []

    def add(src, dst):
        copies.append(pltpu.make_async_copy(src, dst, sems.at[used + len(copies)]))

    cs, cd = pl.ds(start, width), pl.ds(at, width)
    for k, block in enumerate(blocks):
        p = source(order[2], k)
        if order == "xyz":
            add(block.at[:, :, :, cs], whole.at[p & 1, :, :, p >> 1, :, cd])
        else:
            for z in range(4):
                if order == "zxy":
                    add(block.at[:, z, :, cs], whole.at[z & 1, p, :, z >> 1, :, cd])
                else:
                    add(block.at[z, :, :, cs], whole.at[z & 1, :, p, z >> 1, :, cd])
    return copies


def whole_scratch(width):
    return pltpu.VMEM((2, 4, 4, 2, ROWS, width), bf)


def dot(a, b):
    return jnp.dot(a, b, preferred_element_type=jnp.float32)


def dot_t(a, b):
    return lax.dot_general(a, b, (((1,), (1,)), ((), ())), preferred_element_type=jnp.float32)


def both_tokens(own, other, x, sems, used):
    half = own.shape[0]
    return [
        pltpu.make_async_copy(own, x.at[pl.ds(0, half)], sems.at[used]),
        pltpu.make_async_copy(other, x.at[pl.ds(half, half)], sems.at[used + 1]),
    ]


def mixer_kernel(order, own, other, taps, *refs):
    blocks, mixed, x, w, sems = refs[:4], refs[4], refs[5], refs[6], refs[7]
    copies = both_tokens(own, other, x, sems, 0)
    copies += fill(order, blocks, 0, 3 * CHANNELS, w, 0, sems, 2)
    finish(copies)

    def product(i):
        return dot(x[...], w[..., i * CHANNELS : (i + 1) * CHANNELS].reshape(D, CHANNELS))

    gated = product(1) * product(2)
    place = lax.broadcasted_iota(jnp.int32, gated.shape, 0) & (SEQ - 1)
    before = jnp.where(place > 0, pltpu.roll(gated, 1, 0), 0.0)
    after = jnp.where(place < SEQ - 1, pltpu.roll(gated, gated.shape[0] - 1, 0), 0.0)
    conv = taps[0:1] * before + taps[1:2] * gated + taps[2:3] * after
    mixed[...] = (product(0) * conv).astype(bf)


def mixer(order, own, other, taps, blocks):
    rows = 2 * own.shape[0]
    return pl.pallas_call(
        functools.partial(mixer_kernel, order),
        out_shape=jax.ShapeDtypeStruct((rows, CHANNELS), bf),
        in_specs=[HBM, HBM, VMEM] + [HBM] * 4,
        out_specs=VMEM,
        scratch_shapes=[
            pltpu.VMEM((rows, D), bf),
            whole_scratch(3 * CHANNELS),
            pltpu.SemaphoreType.DMA((18,)),
        ],
        compiler_params=PARAMS,
        cost_estimate=pl.CostEstimate(
            flops=2 * rows * D * 3 * CHANNELS, bytes_accessed=8_000_000, transcendentals=0
        ),
    )(own, other, taps, *blocks)


def projected(left, whole, own, other, more=None):
    half = own.shape[0]

    def step(j, _):
        rows = whole[j >> 2, j & 3].reshape(256, whole.shape[-1])
        cols = pl.ds(pl.multiple_of(j * 256, 256), 256)
        sums = dot_t(left[...], rows)
        if more is not None:
            sums = sums + more[:, cols]
        own[:, cols] = sums[:half].astype(own.dtype)
        other[:, cols] = sums[half:].astype(other.dtype)
        return 0

    lax.fori_loop(0, 8, step, 0)


def mix_out_kernel(*refs):
    mixed, blocks = refs[:3], refs[3:15]
    own, other, left, whole, sems = refs[15:]
    copies = []
    for c, order in enumerate(ORDERS):
        at = c * CHANNELS
        part = blocks[4 * c : 4 * c + 4]
        copies += fill(order, part, 3 * CHANNELS, CHANNELS, whole, at, sems, len(copies))
        left[:, at : at + CHANNELS] = mixed[c][...]
    finish(copies)
    projected(left, whole, own, other)


def mix_out_product(mixed, blocks):
    rows = mixed[0].shape[0]
    return pl.pallas_call(
        mix_out_kernel,
        out_shape=[
            jax.ShapeDtypeStruct((rows // 2, D), jnp.float32),
            jax.ShapeDtypeStruct((rows // 2, D), bf),
        ],
        in_specs=[VMEM] * 3 + [HBM] * 12,
        out_specs=[VMEM] * 2,
        scratch_shapes=[
            pltpu.VMEM((rows, 3 * CHANNELS), bf),
            whole_scratch(3 * CHANNELS),
            pltpu.SemaphoreType.DMA((36,)),
        ],
        compiler_params=PARAMS,
        cost_estimate=pl.CostEstimate(
            flops=2 * rows * D * 3 * CHANNELS, bytes_accessed=9_000_000, transcendentals=0
        ),
    )(*mixed, *blocks)


def feed_kernel(first_own, first_other, *refs):
    blocks = refs[:12]
    own, other, x, up, down, hidden, sems = refs[12:]
    tokens = both_tokens(first_own, first_other, x, sems, 0)
    used = 2
    ups, downs = [], []
    for start, whole, sets in ((0, up, ups), (1, down, downs)):
        for c, order in enumerate(ORDERS):
            n = HIDDEN[c]
            part = blocks[4 * c : 4 * c + 4]
            sets.append(fill(order, part, start * n, n, whole, sum(HIDDEN[:c]), sems, used))
            used += len(sets[-1])
    for copy in sum(ups + downs, tokens):
        copy.start()
    for copy in tokens:
        copy.wait()

    def step(j, _):
        cols = pl.ds(pl.multiple_of(j * 256, 256), 256)
        raised = jnp.maximum(dot(x[...], up[..., cols].reshape(D, 256)), 0.0)
        hidden[:, cols] = (raised * raised).astype(bf)
        return 0

    ready = [sum(HIDDEN[: c + 1]) // 256 for c in range(3)]
    for c in range(3):
        for copy in ups[c]:
            copy.wait()
        lax.fori_loop(ready[c - 1] if c else 0, ready[c], step, 0)
    for copy in sum(downs, []):
        copy.wait()
    projected(hidden, down, own, other)


def feed(own, other, blocks):
    rows = 2 * own.shape[0]
    width = sum(HIDDEN)
    return pl.pallas_call(
        feed_kernel,
        out_shape=[
            jax.ShapeDtypeStruct((rows // 2, D), jnp.float32),
            jax.ShapeDtypeStruct((rows // 2, D), bf),
        ],
        in_specs=[HBM] * 14,
        out_specs=[VMEM] * 2,
        scratch_shapes=[
            pltpu.VMEM((rows, D), bf),
            whole_scratch(width),
            whole_scratch(width),
            pltpu.VMEM((rows, width), bf),
            pltpu.SemaphoreType.DMA((80,)),
        ],
        compiler_params=PARAMS,
        cost_estimate=pl.CostEstimate(
            flops=4 * rows * D * width, bytes_accessed=30_000_000, transcendentals=0
        ),
    )(own, other, *blocks)


def joined_kernel(skip, own, other, gain, out):
    def step(i, _):
        rows = pl.ds(pl.multiple_of(i * 16, 16), 16)
        values = residual_scale * skip[rows].astype(jnp.float32)
        values = values + (own[rows] + other[rows].astype(jnp.float32))
        center = values - jnp.mean(values, axis=-1, keepdims=True)
        spread = jnp.mean(center * center, axis=-1, keepdims=True)
        out[rows] = (center * lax.rsqrt(spread + norm_epsilon) * gain[...]).astype(bf)
        return 0

    lax.fori_loop(0, out.shape[0] // 16, step, 0)


def joined(skip, own, other, gain):
    other = swapped(other)
    return pl.pallas_call(
        joined_kernel,
        out_shape=jax.ShapeDtypeStruct(skip.shape, bf),
        in_specs=[VMEM] * 4,
        out_specs=VMEM,
        compiler_params=PARAMS,
    )(skip, own, other, gain.reshape(1, -1))


def local(
    tokens,
    outer_weight,
    inner_weight,
    value_weight,
    conv_taps,
    mix_out,
    norm_first,
    up_weight,
    down_weight,
    norm_second,
):
    parts = pieces(outer_weight, inner_weight, value_weight, mix_out.T, up_weight, down_weight.T)
    tokens_other = swapped(tokens)
    near, far = [], []
    for c, order in enumerate(ORDERS):
        ring = around(parts[c], order[0])
        near.append(placed(ring, order[0], [parts[c].shape[-1]])[0])
    for c, order in enumerate(ORDERS):
        ring = around(near[c], order[1])
        far.append(placed(ring, order[1], stage_widths(c)))
    blocks = [[around(far[c][s], ORDERS[c][2]) for c in range(3)] for s in range(2)]

    mixed = []
    for c, order in enumerate(ORDERS):
        taps = conv_taps[:, c * CHANNELS : (c + 1) * CHANNELS]
        mixed.append(mixer(order, tokens, tokens_other, taps, blocks[0][c]))
    own, other = mix_out_product(mixed, sum(blocks[0], []))
    first = joined(tokens, own, other, norm_first)
    first_other = swapped(first)
    own, other = feed(first, first_other, sum(blocks[1], []))
    return joined(first, own, other, norm_second)


def solution(mesh):
    finer = Mesh(
        mesh.devices.reshape(2, 2, 4, 4, 2),
        ("rep", "fs_0", "fs_1", "fs_2", "tp"),
    )
    placement = (
        P(REP_FS_TP, None),
        P(FS, "tp"),
        P(FS, "tp"),
        P(FS, "tp"),
        P(None, "tp"),
        P("tp", FS),
        P(),
        P(FS, "tp"),
        P("tp", FS),
        P(),
    )
    return jax.shard_map(
        local, mesh=finer, in_specs=placement, out_specs=P(REP_FS_TP, None), check_vma=False
    )
```

```python
import functools

import jax
import jax.numpy as jnp
from jax import lax
from jax.experimental import pallas as pl
from jax.experimental.pallas import tpu as pltpu
from jax.sharding import Mesh
from jax.sharding import PartitionSpec as P


SEQ = 128
D = 2048
ROWS = 32
FS = ("fs_0", "fs_1", "fs_2")
REP_FS_TP = ("rep", "fs_0", "fs_1", "fs_2", "tp")
ORDERS = ("zxy", "xyz", "yzx")
CHANNELS = 256
HIDDEN = (768, 640, 640)


residual_scale = 2.0**0.25
norm_epsilon = 1e-05
bf = jnp.bfloat16
HBM = pl.BlockSpec(memory_space=pltpu.HBM)
VMEM = pl.BlockSpec(memory_space=pltpu.VMEM)


def limit(mebibytes):
    return pltpu.CompilerParams(vmem_limit_bytes=mebibytes * 1024 * 1024)


def in_hbm(arrays):
    return [pltpu.with_memory_space_constraint(a, pltpu.HBM) for a in arrays]


def stage_widths(part):
    return [4 * CHANNELS, 2 * HIDDEN[part]]


def position(axis):
    if axis == "z":
        return lax.axis_index("rep") * 2 + lax.axis_index("fs_0")
    return lax.axis_index({"y": "fs_1", "x": "fs_2"}[axis])


def source(axis, step):
    way = 2 * lax.axis_index("tp") - 1
    return (position(axis) + 4 + way * step) & 3


def ring_pairs(axis, step):
    at = "zyx".index(axis)
    pairs = []
    for z in range(4):
        for y in range(4):
            for x in range(4):
                for core in range(2):
                    to = [z, y, x]
                    to[at] = (to[at] + (step if core == 0 else 4 - step)) % 4
                    start = ((z * 4 + y) * 4 + x) * 2 + core
                    pairs.append((start, ((to[0] * 4 + to[1]) * 4 + to[2]) * 2 + core))
    return pairs


def moved(block, axis, step):
    return lax.ppermute(block, REP_FS_TP, ring_pairs(axis, step))


def around(block, axis):
    near, back = moved(block, axis, 1), moved(block, axis, 3)
    return [block, near, moved(near, axis, 1), back]


def swapped(x):
    return lax.ppermute(x, "tp", [(0, 1), (1, 0)])


def finish(copies):
    for copy in copies:
        copy.start()
    for copy in copies:
        copy.wait()


def pieces_kernel(*refs):
    weights, outs, held, sems = refs[:6], refs[6:9], refs[9:15], refs[15]
    rows = pl.ds(lax.axis_index("rep") * ROWS, ROWS)
    finish(
        [
            pltpu.make_async_copy(w.at[rows], h, sems.at[i])
            for i, (w, h) in enumerate(zip(weights, held))
        ]
    )
    outer, inner, value, mix, up, down = held
    for part, out in enumerate(outs):
        at = 0
        for w in (outer, inner, value, mix):
            out[:, at : at + CHANNELS] = w[:, part * CHANNELS : (part + 1) * CHANNELS].astype(bf)
            at += CHANNELS
        start, n = sum(HIDDEN[:part]), HIDDEN[part]
        for w in (up, down):
            out[:, at : at + n] = w[:, start : start + n].astype(bf)
            at += n


def pieces(*weights):
    return pl.pallas_call(
        pieces_kernel,
        out_shape=[jax.ShapeDtypeStruct((ROWS, sum(stage_widths(c))), bf) for c in range(3)],
        in_specs=[HBM] * 6,
        out_specs=[VMEM] * 3,
        scratch_shapes=[pltpu.VMEM((ROWS, w.shape[1]), jnp.float32) for w in weights]
        + [pltpu.SemaphoreType.DMA((6,))],
        compiler_params=limit(6),
    )(*in_hbm(weights))


def place_kernel(axis, start, *refs):
    parts, out, sems = refs[:4], refs[4], refs[5]
    width = out.shape[-1]
    finish(
        [
            pltpu.make_async_copy(
                part.at[..., pl.ds(start, width)], out.at[source(axis, k)], sems.at[k]
            )
            for k, part in enumerate(parts)
        ]
    )


def placed(parts, axis, start, width):
    return pl.pallas_call(
        functools.partial(place_kernel, axis, start),
        out_shape=pltpu.HBM((4, *parts[0].shape[:-1], width), bf),
        in_specs=[HBM] * 4,
        out_specs=HBM,
        scratch_shapes=[pltpu.SemaphoreType.DMA((4,))],
        compiler_params=limit(4),
    )(*parts)


def fill(order, blocks, start, width, whole, at, sems, used):
    copies = []

    def add(src, dst):
        copies.append(pltpu.make_async_copy(src, dst, sems.at[used + len(copies)]))

    cs, cd = pl.ds(start, width), pl.ds(at, width)
    for k, block in enumerate(blocks):
        p = source(order[2], k)
        if order == "xyz":
            add(block.at[:, :, :, cs], whole.at[p & 1, :, :, p >> 1, :, cd])
        else:
            for z in range(4):
                if order == "zxy":
                    add(block.at[:, z, :, cs], whole.at[z & 1, p, :, z >> 1, :, cd])
                else:
                    add(block.at[z, :, :, cs], whole.at[z & 1, :, p, z >> 1, :, cd])
    return copies


def whole_scratch(width):
    return pltpu.VMEM((2, 4, 4, 2, ROWS, width), bf)


def dot(a, b):
    return jnp.dot(a, b, preferred_element_type=jnp.float32)


def dot_t(a, b):
    return lax.dot_general(a, b, (((1,), (1,)), ((), ())), preferred_element_type=jnp.float32)


def both_tokens(own, other, x, sems, used):
    half = own.shape[0]
    return [
        pltpu.make_async_copy(own, x.at[pl.ds(0, half)], sems.at[used]),
        pltpu.make_async_copy(other, x.at[pl.ds(half, half)], sems.at[used + 1]),
    ]


def mixer_kernel(order, own, other, taps, *refs):
    blocks, mixed, x, w, sems = refs[:4], refs[4], refs[5], refs[6], refs[7]
    copies = both_tokens(own, other, x, sems, 0)
    copies += fill(order, blocks, 0, 3 * CHANNELS, w, 0, sems, 2)
    finish(copies)

    def product(i):
        return dot(x[...], w[..., i * CHANNELS : (i + 1) * CHANNELS].reshape(D, CHANNELS))

    gated = product(1) * product(2)
    place = lax.broadcasted_iota(jnp.int32, gated.shape, 0) & (SEQ - 1)
    before = jnp.where(place > 0, pltpu.roll(gated, 1, 0), 0.0)
    after = jnp.where(place < SEQ - 1, pltpu.roll(gated, gated.shape[0] - 1, 0), 0.0)
    conv = taps[0:1] * before + taps[1:2] * gated + taps[2:3] * after
    mixed[...] = (product(0) * conv).astype(bf)


def mixer(order, own, other, taps, blocks):
    rows = 2 * own.shape[0]
    return pl.pallas_call(
        functools.partial(mixer_kernel, order),
        out_shape=jax.ShapeDtypeStruct((rows, CHANNELS), bf),
        in_specs=[HBM, HBM, VMEM] + [HBM] * 4,
        out_specs=VMEM,
        scratch_shapes=[
            pltpu.VMEM((rows, D), bf),
            whole_scratch(3 * CHANNELS),
            pltpu.SemaphoreType.DMA((18,)),
        ],
        compiler_params=limit(16),
        cost_estimate=pl.CostEstimate(
            flops=2 * rows * D * 3 * CHANNELS, bytes_accessed=8_000_000, transcendentals=0
        ),
    )(own, other, taps, *blocks)


def projected(left, whole, own, other, more=None):
    half = own.shape[0]

    def step(j, _):
        rows = whole[j >> 2, j & 3].reshape(256, whole.shape[-1])
        cols = pl.ds(pl.multiple_of(j * 256, 256), 256)
        sums = dot_t(left[...], rows)
        ours, theirs = sums[:half], sums[half:]
        if more is not None:
            ours, theirs = ours + more[0][:, cols], theirs + more[1][:, cols]
        own[:, cols] = ours.astype(own.dtype)
        other[:, cols] = theirs.astype(other.dtype)
        return 0

    lax.fori_loop(0, 8, step, 0)


def mix_out_kernel(*refs):
    mixed, blocks = refs[:3], refs[3:15]
    own, other, left, whole, sems = refs[15:]
    copies = []
    for c, order in enumerate(ORDERS):
        at = c * CHANNELS
        part = blocks[4 * c : 4 * c + 4]
        copies += fill(order, part, 3 * CHANNELS, CHANNELS, whole, at, sems, len(copies))
        left[:, at : at + CHANNELS] = mixed[c][...]
    finish(copies)
    projected(left, whole, own, other)


def mix_out_product(mixed, blocks):
    rows = mixed[0].shape[0]
    return pl.pallas_call(
        mix_out_kernel,
        out_shape=[
            jax.ShapeDtypeStruct((rows // 2, D), jnp.float32),
            jax.ShapeDtypeStruct((rows // 2, D), bf),
        ],
        in_specs=[VMEM] * 3 + [HBM] * 12,
        out_specs=[VMEM] * 2,
        scratch_shapes=[
            pltpu.VMEM((rows, 3 * CHANNELS), bf),
            whole_scratch(3 * CHANNELS),
            pltpu.SemaphoreType.DMA((36,)),
        ],
        compiler_params=limit(16),
        cost_estimate=pl.CostEstimate(
            flops=2 * rows * D * 3 * CHANNELS, bytes_accessed=9_000_000, transcendentals=0
        ),
    )(*mixed, *blocks)


def feed_kernel(parts, first_own, first_other, *refs):
    blocks, refs = refs[: 4 * len(parts)], refs[4 * len(parts) :]
    more = None
    if len(refs) == 9:
        more, refs = refs[:2], refs[2:]
    own, other, x, up, down, hidden, sems = refs
    tokens = both_tokens(first_own, first_other, x, sems, 0)
    used = 2
    ends = [sum(HIDDEN[c] for c in parts[: i + 1]) for i in range(len(parts))]
    ups, downs = [], []
    for second, whole, sets in ((0, up, ups), (1, down, downs)):
        for i, c in enumerate(parts):
            n = HIDDEN[c]
            ring = blocks[4 * i : 4 * i + 4]
            sets.append(fill(ORDERS[c], ring, second * n, n, whole, ends[i] - n, sems, used))
            used += len(sets[-1])
    for copy in sum(ups + downs, tokens):
        copy.start()
    for copy in tokens:
        copy.wait()

    def step(j, _):
        cols = pl.ds(pl.multiple_of(j * 256, 256), 256)
        raised = jnp.maximum(dot(x[...], up[..., cols].reshape(D, 256)), 0.0)
        hidden[:, cols] = (raised * raised).astype(bf)
        return 0

    done = 0
    for copies, end in zip(ups, ends):
        for copy in copies:
            copy.wait()
        lax.fori_loop(done, end // 256, step, 0)
        done = end // 256
    for copy in sum(downs, []):
        copy.wait()
    projected(hidden, down, own, other, more)


def feed(parts, own, other, blocks, more=None):
    half = own.shape[0]
    width = sum(HIDDEN[c] for c in parts)
    extra = [] if more is None else list(more)
    last = jnp.float32 if more is None else bf
    return pl.pallas_call(
        functools.partial(feed_kernel, parts),
        out_shape=[
            jax.ShapeDtypeStruct((half, D), jnp.float32),
            jax.ShapeDtypeStruct((half, D), last),
        ],
        in_specs=[HBM] * (2 + len(blocks)) + [VMEM] * len(extra),
        out_specs=[VMEM] * 2,
        scratch_shapes=[
            pltpu.VMEM((2 * half, D), bf),
            whole_scratch(width),
            whole_scratch(width),
            pltpu.VMEM((2 * half, width), bf),
            pltpu.SemaphoreType.DMA((80,)),
        ],
        compiler_params=limit(32),
        cost_estimate=pl.CostEstimate(
            flops=8 * half * D * width, bytes_accessed=20_000_000, transcendentals=0
        ),
    )(own, other, *blocks, *extra)


def joined_kernel(skip, own, other, gain, out):
    def step(i, _):
        rows = pl.ds(pl.multiple_of(i * 128, 128), 128)
        values = residual_scale * skip[rows].astype(jnp.float32)
        values = values + (own[rows] + other[rows].astype(jnp.float32))
        center = values - jnp.mean(values, axis=-1, keepdims=True)
        spread = jnp.mean(center * center, axis=-1, keepdims=True)
        out[rows] = (center * lax.rsqrt(spread + norm_epsilon) * gain[...]).astype(bf)
        return 0

    lax.fori_loop(0, out.shape[0] // 128, step, 0)


def joined(skip, own, other, gain):
    other = swapped(other)
    return pl.pallas_call(
        joined_kernel,
        out_shape=jax.ShapeDtypeStruct(skip.shape, bf),
        in_specs=[VMEM] * 4,
        out_specs=VMEM,
        compiler_params=limit(16),
    )(skip, own, other, gain.reshape(1, -1))


def local(
    tokens,
    outer_weight,
    inner_weight,
    value_weight,
    conv_taps,
    mix_out,
    norm_first,
    up_weight,
    down_weight,
    norm_second,
):
    parts = pieces(outer_weight, inner_weight, value_weight, mix_out.T, up_weight, down_weight.T)
    tokens_other = swapped(tokens)
    near, far = [], []
    for c, order in enumerate(ORDERS):
        ring = around(parts[c], order[0])
        near.append(placed(ring, order[0], 0, parts[c].shape[-1]))
    for c, order in enumerate(ORDERS):
        ring = around(near[c], order[1])
        both = []
        for s, width in enumerate(stage_widths(c)):
            both.append(placed(ring, order[1], s * 4 * CHANNELS, width))
        far.append(both)
    blocks = [[around(far[c][s], ORDERS[c][2]) for c in range(3)] for s in range(2)]

    mixed = []
    for c, order in enumerate(ORDERS):
        taps = conv_taps[:, c * CHANNELS : (c + 1) * CHANNELS]
        mixed.append(mixer(order, tokens, tokens_other, taps, blocks[0][c]))
    own, other = mix_out_product(mixed, sum(blocks[0], []))
    first = joined(tokens, own, other, norm_first)
    first_other = swapped(first)
    sums = feed((0,), first, first_other, blocks[1][0])
    own, other = feed((1, 2), first, first_other, blocks[1][1] + blocks[1][2], sums)
    return joined(first, own, other, norm_second)


def solution(mesh):
    finer = Mesh(
        mesh.devices.reshape(2, 2, 4, 4, 2),
        ("rep", "fs_0", "fs_1", "fs_2", "tp"),
    )
    placement = (
        P(REP_FS_TP, None),
        P(FS, "tp"),
        P(FS, "tp"),
        P(FS, "tp"),
        P(None, "tp"),
        P("tp", FS),
        P(),
        P(FS, "tp"),
        P("tp", FS),
        P(),
    )
    return jax.shard_map(
        local, mesh=finer, in_specs=placement, out_specs=P(REP_FS_TP, None), check_vma=False
    )
```

```python
import functools

import jax
import jax.numpy as jnp
from jax import lax
from jax.experimental import pallas as pl
from jax.experimental.pallas import tpu as pltpu
from jax.sharding import Mesh
from jax.sharding import PartitionSpec as P


SEQ = 128
D = 2048
ROWS = 32
FS = ("fs_0", "fs_1", "fs_2")
REP_FS_TP = ("rep", "fs_0", "fs_1", "fs_2", "tp")
ORDERS = ("zxy", "xyz", "yzx")
CHANNELS = 256
HIDDEN = ((384, 384, 256), (384, 256, 384))


residual_scale = 2.0**0.25
norm_epsilon = 1e-05
bf = jnp.bfloat16
HBM = pl.BlockSpec(memory_space=pltpu.HBM)
VMEM = pl.BlockSpec(memory_space=pltpu.VMEM)


def limit(mebibytes):
    return pltpu.CompilerParams(vmem_limit_bytes=mebibytes * 1024 * 1024)


def in_hbm(arrays):
    return [pltpu.with_memory_space_constraint(a, pltpu.HBM) for a in arrays]


def stage_widths(part):
    return [4 * CHANNELS] + [2 * HIDDEN[s][part] for s in range(2)]


def position(axis):
    if axis == "z":
        return lax.axis_index("rep") * 2 + lax.axis_index("fs_0")
    return lax.axis_index({"y": "fs_1", "x": "fs_2"}[axis])


def source(axis, step):
    way = 2 * lax.axis_index("tp") - 1
    return (position(axis) + 4 + way * step) & 3


def ring_pairs(axis, step):
    at = "zyx".index(axis)
    pairs = []
    for z in range(4):
        for y in range(4):
            for x in range(4):
                for core in range(2):
                    to = [z, y, x]
                    to[at] = (to[at] + (step if core == 0 else 4 - step)) % 4
                    start = ((z * 4 + y) * 4 + x) * 2 + core
                    pairs.append((start, ((to[0] * 4 + to[1]) * 4 + to[2]) * 2 + core))
    return pairs


def moved(block, axis, step):
    return lax.ppermute(block, REP_FS_TP, ring_pairs(axis, step))


def around(block, axis):
    near, back = moved(block, axis, 1), moved(block, axis, 3)
    return [block, near, moved(near, axis, 1), back]


def swapped(x):
    return lax.ppermute(x, "tp", [(0, 1), (1, 0)])


def finish(copies):
    for copy in copies:
        copy.start()
    for copy in copies:
        copy.wait()


def pieces_kernel(*refs):
    weights, outs, held, sems = refs[:6], refs[6:9], refs[9:15], refs[15]
    rows = pl.ds(lax.axis_index("rep") * ROWS, ROWS)
    finish(
        [
            pltpu.make_async_copy(w.at[rows], h, sems.at[i])
            for i, (w, h) in enumerate(zip(weights, held))
        ]
    )
    outer, inner, value, mix, up, down = held
    for part, out in enumerate(outs):
        at = 0
        for w in (outer, inner, value, mix):
            out[:, at : at + CHANNELS] = w[:, part * CHANNELS : (part + 1) * CHANNELS].astype(bf)
            at += CHANNELS
        for s in range(2):
            start, n = s * sum(HIDDEN[0]) + sum(HIDDEN[s][:part]), HIDDEN[s][part]
            for w in (up, down):
                out[:, at : at + n] = w[:, start : start + n].astype(bf)
                at += n


def pieces(*weights):
    return pl.pallas_call(
        pieces_kernel,
        out_shape=[jax.ShapeDtypeStruct((ROWS, sum(stage_widths(c))), bf) for c in range(3)],
        in_specs=[HBM] * 6,
        out_specs=[VMEM] * 3,
        scratch_shapes=[pltpu.VMEM((ROWS, w.shape[1]), jnp.float32) for w in weights]
        + [pltpu.SemaphoreType.DMA((6,))],
        compiler_params=limit(6),
    )(*in_hbm(weights))


def place_kernel(axis, columns, *refs):
    parts, outs, sems = refs[:4], refs[4:-1], refs[-1]
    copies = []
    for k, part in enumerate(parts):
        for (start, width), out in zip(columns, outs):
            src, dst = part.at[..., pl.ds(start, width)], out.at[source(axis, k)]
            copies.append(pltpu.make_async_copy(src, dst, sems.at[len(copies)]))
    finish(copies)


def placed(parts, axis, columns):
    lead = parts[0].shape[:-1]
    return pl.pallas_call(
        functools.partial(place_kernel, axis, columns),
        out_shape=[pltpu.HBM((4, *lead, width), bf) for _, width in columns],
        in_specs=[HBM] * 4,
        out_specs=[HBM] * len(columns),
        scratch_shapes=[pltpu.SemaphoreType.DMA((4 * len(columns),))],
        compiler_params=limit(4),
    )(*parts)


def fill(order, blocks, start, width, whole, at, sems, used, shift=0):
    copies = []

    def add(src, dst):
        copies.append(pltpu.make_async_copy(src, dst, sems.at[used + len(copies)]))

    cd = pl.ds(at, width)
    for k, block in enumerate(blocks):
        p = source(order[2], k)
        cs = pl.ds(start + (shift if k == 3 else 0), width)
        if order == "xyz":
            add(block.at[:, :, :, cs], whole.at[p & 1, :, :, p >> 1, :, cd])
        else:
            for z in range(4):
                if order == "zxy":
                    add(block.at[:, z, :, cs], whole.at[z & 1, p, :, z >> 1, :, cd])
                else:
                    add(block.at[z, :, :, cs], whole.at[z & 1, :, p, z >> 1, :, cd])
    return copies


def whole_scratch(width):
    return pltpu.VMEM((2, 4, 4, 2, ROWS, width), bf)


def dot(a, b):
    return jnp.dot(a, b, preferred_element_type=jnp.float32)


def dot_t(a, b):
    return lax.dot_general(a, b, (((1,), (1,)), ((), ())), preferred_element_type=jnp.float32)


def both_tokens(own, other, x, sems, used):
    half = own.shape[0]
    return [
        pltpu.make_async_copy(own, x.at[pl.ds(0, half)], sems.at[used]),
        pltpu.make_async_copy(other, x.at[pl.ds(half, half)], sems.at[used + 1]),
    ]


def mixer_kernel(order, own, other, taps, *refs):
    blocks, mixed, x, w, sems = refs[:4], refs[4], refs[5], refs[6], refs[7]
    copies = both_tokens(own, other, x, sems, 0)
    copies += fill(order, blocks, 0, 3 * CHANNELS, w, 0, sems, 2)
    finish(copies)

    def product(i):
        return dot(x[...], w[..., i * CHANNELS : (i + 1) * CHANNELS].reshape(D, CHANNELS))

    gated = product(1) * product(2)
    place = lax.broadcasted_iota(jnp.int32, gated.shape, 0) & (SEQ - 1)
    before = jnp.where(place > 0, pltpu.roll(gated, 1, 0), 0.0)
    after = jnp.where(place < SEQ - 1, pltpu.roll(gated, gated.shape[0] - 1, 0), 0.0)
    conv = taps[0:1] * before + taps[1:2] * gated + taps[2:3] * after
    mixed[...] = (product(0) * conv).astype(bf)


def mixer(order, own, other, taps, blocks):
    rows = 2 * own.shape[0]
    return pl.pallas_call(
        functools.partial(mixer_kernel, order),
        out_shape=jax.ShapeDtypeStruct((rows, CHANNELS), bf),
        in_specs=[HBM, HBM, VMEM] + [HBM] * 4,
        out_specs=VMEM,
        scratch_shapes=[
            pltpu.VMEM((rows, D), bf),
            whole_scratch(3 * CHANNELS),
            pltpu.SemaphoreType.DMA((18,)),
        ],
        compiler_params=limit(16),
        cost_estimate=pl.CostEstimate(
            flops=2 * rows * D * 3 * CHANNELS, bytes_accessed=8_000_000, transcendentals=0
        ),
    )(own, other, taps, *blocks)


def projected(left, whole, own, other, more=None):
    half = own.shape[0]

    def step(j, _):
        rows = whole[j >> 2, j & 3].reshape(256, whole.shape[-1])
        cols = pl.ds(pl.multiple_of(j * 256, 256), 256)
        sums = dot_t(left[...], rows)
        ours, theirs = sums[:half], sums[half:]
        if more is not None:
            ours, theirs = ours + more[0][:, cols], theirs + more[1][:, cols]
        own[:, cols] = ours.astype(own.dtype)
        other[:, cols] = theirs.astype(other.dtype)
        return 0

    lax.fori_loop(0, 8, step, 0)


def mix_out_kernel(*refs):
    mixed, blocks = refs[:3], refs[3:15]
    own, other, left, whole, sems = refs[15:]
    copies = []
    for c, order in enumerate(ORDERS):
        at = c * CHANNELS
        part = blocks[4 * c : 4 * c + 4]
        copies += fill(order, part, 3 * CHANNELS, CHANNELS, whole, at, sems, len(copies))
        left[:, at : at + CHANNELS] = mixed[c][...]
    finish(copies)
    projected(left, whole, own, other)


def mix_out_product(mixed, blocks):
    rows = mixed[0].shape[0]
    return pl.pallas_call(
        mix_out_kernel,
        out_shape=[
            jax.ShapeDtypeStruct((rows // 2, D), jnp.float32),
            jax.ShapeDtypeStruct((rows // 2, D), bf),
        ],
        in_specs=[VMEM] * 3 + [HBM] * 12,
        out_specs=[VMEM] * 2,
        scratch_shapes=[
            pltpu.VMEM((rows, 3 * CHANNELS), bf),
            whole_scratch(3 * CHANNELS),
            pltpu.SemaphoreType.DMA((36,)),
        ],
        compiler_params=limit(16),
        cost_estimate=pl.CostEstimate(
            flops=2 * rows * D * 3 * CHANNELS, bytes_accessed=9_000_000, transcendentals=0
        ),
    )(*mixed, *blocks)


def feed_kernel(stage, first_own, first_other, *refs):
    blocks, refs = refs[:12], refs[12:]
    more = None
    if len(refs) == 9:
        more, refs = refs[:2], refs[2:]
    own, other, x, up, down, hidden, sems = refs
    tokens = both_tokens(first_own, first_other, x, sems, 0)
    used = 2
    ends = [sum(HIDDEN[stage][: c + 1]) for c in range(3)]
    ups, downs = [], []
    for second, whole, sets in ((0, up, ups), (1, down, downs)):
        for c, order in enumerate(ORDERS):
            n = HIDDEN[stage][c]
            ring = blocks[4 * c : 4 * c + 4]
            shift = stage * 2 * HIDDEN[0][c]
            sets.append(fill(order, ring, second * n, n, whole, ends[c] - n, sems, used, shift))
            used += len(sets[-1])
    for copy in sum(ups + downs, tokens):
        copy.start()
    for copy in tokens:
        copy.wait()

    def step(j, _):
        cols = pl.ds(pl.multiple_of(j * 256, 256), 256)
        raised = jnp.maximum(dot(x[...], up[..., cols].reshape(D, 256)), 0.0)
        hidden[:, cols] = (raised * raised).astype(bf)
        return 0

    done = 0
    for copies, end in zip(ups, ends):
        for copy in copies:
            copy.wait()
        lax.fori_loop(done, end // 256, step, 0)
        done = end // 256
    for copy in sum(downs, []):
        copy.wait()
    projected(hidden, down, own, other, more)


def feed(stage, own, other, blocks, more=None):
    half = own.shape[0]
    width = sum(HIDDEN[stage])
    extra = [] if more is None else list(more)
    last = jnp.float32 if more is None else bf
    return pl.pallas_call(
        functools.partial(feed_kernel, stage),
        out_shape=[
            jax.ShapeDtypeStruct((half, D), jnp.float32),
            jax.ShapeDtypeStruct((half, D), last),
        ],
        in_specs=[HBM] * (2 + len(blocks)) + [VMEM] * len(extra),
        out_specs=[VMEM] * 2,
        scratch_shapes=[
            pltpu.VMEM((2 * half, D), bf),
            whole_scratch(width),
            whole_scratch(width),
            pltpu.VMEM((2 * half, width), bf),
            pltpu.SemaphoreType.DMA((80,)),
        ],
        compiler_params=limit(32),
        cost_estimate=pl.CostEstimate(
            flops=8 * half * D * width, bytes_accessed=20_000_000, transcendentals=0
        ),
    )(own, other, *blocks, *extra)


def joined_kernel(skip, own, other, gain, out):
    def step(i, _):
        rows = pl.ds(pl.multiple_of(i * 128, 128), 128)
        values = residual_scale * skip[rows].astype(jnp.float32)
        values = values + (own[rows] + other[rows].astype(jnp.float32))
        center = values - jnp.mean(values, axis=-1, keepdims=True)
        spread = jnp.mean(center * center, axis=-1, keepdims=True)
        out[rows] = (center * lax.rsqrt(spread + norm_epsilon) * gain[...]).astype(bf)
        return 0

    lax.fori_loop(0, out.shape[0] // 128, step, 0)


def joined(skip, own, other, gain):
    other = swapped(other)
    return pl.pallas_call(
        joined_kernel,
        out_shape=jax.ShapeDtypeStruct(skip.shape, bf),
        in_specs=[VMEM] * 4,
        out_specs=VMEM,
        compiler_params=limit(16),
    )(skip, own, other, gain.reshape(1, -1))


def local(
    tokens,
    outer_weight,
    inner_weight,
    value_weight,
    conv_taps,
    mix_out,
    norm_first,
    up_weight,
    down_weight,
    norm_second,
):
    parts = pieces(outer_weight, inner_weight, value_weight, mix_out.T, up_weight, down_weight.T)
    tokens_other = swapped(tokens)
    near = []
    for c, order in enumerate(ORDERS):
        ring = around(parts[c], order[0])
        near += placed(ring, order[0], [(0, parts[c].shape[-1])])
    blocks = [[], [], []]
    for c, order in enumerate(ORDERS):
        ring = around(near[c], order[1])
        head, one, two = stage_widths(c)
        (own,) = placed(ring, order[1], [(0, head)])
        columns = [(head, one), (head + one, two), (head, one + two)]
        *own_stages, own_both = placed(ring, order[1], columns)
        blocks[0] += around(own, order[2])
        back = moved(own_both, order[2], 3)
        for s, own in enumerate(own_stages, 1):
            ahead = moved(own, order[2], 1)
            blocks[s] += [own, ahead, moved(ahead, order[2], 1), back]

    mixed = []
    for c, order in enumerate(ORDERS):
        taps = conv_taps[:, c * CHANNELS : (c + 1) * CHANNELS]
        mixed.append(mixer(order, tokens, tokens_other, taps, blocks[0][4 * c : 4 * c + 4]))
    own, other = mix_out_product(mixed, blocks[0])
    first = joined(tokens, own, other, norm_first)
    first_other = swapped(first)
    sums = feed(0, first, first_other, blocks[1])
    own, other = feed(1, first, first_other, blocks[2], sums)
    return joined(first, own, other, norm_second)


def solution(mesh):
    finer = Mesh(
        mesh.devices.reshape(2, 2, 4, 4, 2),
        ("rep", "fs_0", "fs_1", "fs_2", "tp"),
    )
    placement = (
        P(REP_FS_TP, None),
        P(FS, "tp"),
        P(FS, "tp"),
        P(FS, "tp"),
        P(None, "tp"),
        P("tp", FS),
        P(),
        P(FS, "tp"),
        P("tp", FS),
        P(),
    )
    return jax.shard_map(
        local, mesh=finer, in_specs=placement, out_specs=P(REP_FS_TP, None), check_vma=False
    )
```

```python
import functools

import jax
import jax.numpy as jnp
from jax import lax
from jax.experimental import pallas as pl
from jax.experimental.pallas import tpu as pltpu
from jax.sharding import Mesh
from jax.sharding import PartitionSpec as P


SEQ = 128
D = 2048
ROWS = 32
FS = ("fs_0", "fs_1", "fs_2")
REP_FS_TP = ("rep", "fs_0", "fs_1", "fs_2", "tp")
ORDERS = ("zxy", "xyz", "yzx")
CHANNELS = 256
HIDDEN = 1024
UPS = ((384, 384, 256), (384, 384, 256))
DOWNS = ((256, 384, 384), (384, 256, 384))


residual_scale = 2.0**0.25
norm_epsilon = 1e-05
bf = jnp.bfloat16
HBM = pl.BlockSpec(memory_space=pltpu.HBM)
VMEM = pl.BlockSpec(memory_space=pltpu.VMEM)


def limit(mebibytes):
    return pltpu.CompilerParams(vmem_limit_bytes=mebibytes * 1024 * 1024)


def in_hbm(arrays):
    return [pltpu.with_memory_space_constraint(a, pltpu.HBM) for a in arrays]


def stage_widths(part):
    return [4 * CHANNELS] + [UPS[s][part] + DOWNS[s][part] for s in range(2)]


def position(axis):
    if axis == "z":
        return lax.axis_index("rep") * 2 + lax.axis_index("fs_0")
    return lax.axis_index({"y": "fs_1", "x": "fs_2"}[axis])


def source(axis, step):
    way = 2 * lax.axis_index("tp") - 1
    return (position(axis) + 4 + way * step) & 3


def ring_pairs(axis, step):
    at = "zyx".index(axis)
    pairs = []
    for z in range(4):
        for y in range(4):
            for x in range(4):
                for core in range(2):
                    to = [z, y, x]
                    to[at] = (to[at] + (step if core == 0 else 4 - step)) % 4
                    start = ((z * 4 + y) * 4 + x) * 2 + core
                    pairs.append((start, ((to[0] * 4 + to[1]) * 4 + to[2]) * 2 + core))
    return pairs


def moved(block, axis, step):
    return lax.ppermute(block, REP_FS_TP, ring_pairs(axis, step))


def around(block, axis):
    near, back = moved(block, axis, 1), moved(block, axis, 3)
    return [block, near, moved(near, axis, 1), back]


def swapped(x):
    return lax.ppermute(x, "tp", [(0, 1), (1, 0)])


def finish(copies):
    for copy in copies:
        copy.start()
    for copy in copies:
        copy.wait()


def pieces_kernel(*refs):
    weights, outs, held, sems = refs[:6], refs[6:9], refs[9:15], refs[15]
    rows = pl.ds(lax.axis_index("rep") * ROWS, ROWS)
    finish(
        [
            pltpu.make_async_copy(w.at[rows], h, sems.at[i])
            for i, (w, h) in enumerate(zip(weights, held))
        ]
    )
    outer, inner, value, mix, up, down = held
    for part, out in enumerate(outs):
        at = 0
        for w in (outer, inner, value, mix):
            out[:, at : at + CHANNELS] = w[:, part * CHANNELS : (part + 1) * CHANNELS].astype(bf)
            at += CHANNELS
        for s in range(2):
            for w, shares in ((up, UPS[s]), (down, DOWNS[s])):
                start, n = s * HIDDEN + sum(shares[:part]), shares[part]
                out[:, at : at + n] = w[:, start : start + n].astype(bf)
                at += n


def pieces(*weights):
    return pl.pallas_call(
        pieces_kernel,
        out_shape=[jax.ShapeDtypeStruct((ROWS, sum(stage_widths(c))), bf) for c in range(3)],
        in_specs=[HBM] * 6,
        out_specs=[VMEM] * 3,
        scratch_shapes=[pltpu.VMEM((ROWS, w.shape[1]), jnp.float32) for w in weights]
        + [pltpu.SemaphoreType.DMA((6,))],
        compiler_params=limit(6),
    )(*in_hbm(weights))


def place_kernel(axis, columns, *refs):
    parts, outs, sems = refs[:4], refs[4:-1], refs[-1]
    copies = []
    for k, part in enumerate(parts):
        for (start, width), out in zip(columns, outs):
            src, dst = part.at[..., pl.ds(start, width)], out.at[source(axis, k)]
            copies.append(pltpu.make_async_copy(src, dst, sems.at[len(copies)]))
    finish(copies)


def placed(parts, axis, columns):
    lead = parts[0].shape[:-1]
    return pl.pallas_call(
        functools.partial(place_kernel, axis, columns),
        out_shape=[pltpu.HBM((4, *lead, width), bf) for _, width in columns],
        in_specs=[HBM] * 4,
        out_specs=[HBM] * len(columns),
        scratch_shapes=[pltpu.SemaphoreType.DMA((4 * len(columns),))],
        compiler_params=limit(4),
    )(*parts)


def fill(order, blocks, start, width, whole, at, sems, used, shift=0):
    copies = []

    def add(src, dst):
        copies.append(pltpu.make_async_copy(src, dst, sems.at[used + len(copies)]))

    cd = pl.ds(at, width)
    for k, block in enumerate(blocks):
        p = source(order[2], k)
        cs = pl.ds(start + (shift if k == 3 else 0), width)
        if order == "xyz":
            add(block.at[:, :, :, cs], whole.at[p & 1, :, :, p >> 1, :, cd])
        else:
            for z in range(4):
                if order == "zxy":
                    add(block.at[:, z, :, cs], whole.at[z & 1, p, :, z >> 1, :, cd])
                else:
                    add(block.at[z, :, :, cs], whole.at[z & 1, :, p, z >> 1, :, cd])
    return copies


def whole_scratch(width):
    return pltpu.VMEM((2, 4, 4, 2, ROWS, width), bf)


def dot(a, b):
    return jnp.dot(a, b, preferred_element_type=jnp.float32)


def dot_t(a, b):
    return lax.dot_general(a, b, (((1,), (1,)), ((), ())), preferred_element_type=jnp.float32)


def both_tokens(own, other, x, sems, used):
    half = own.shape[0]
    return [
        pltpu.make_async_copy(own, x.at[pl.ds(0, half)], sems.at[used]),
        pltpu.make_async_copy(other, x.at[pl.ds(half, half)], sems.at[used + 1]),
    ]


def mixer_kernel(order, own, other, taps, *refs):
    blocks, mixed, x, w, sems = refs[:4], refs[4], refs[5], refs[6], refs[7]
    copies = both_tokens(own, other, x, sems, 0)
    copies += fill(order, blocks, 0, 3 * CHANNELS, w, 0, sems, 2)
    finish(copies)

    def product(i):
        return dot(x[...], w[..., i * CHANNELS : (i + 1) * CHANNELS].reshape(D, CHANNELS))

    gated = product(1) * product(2)
    place = lax.broadcasted_iota(jnp.int32, gated.shape, 0) & (SEQ - 1)
    before = jnp.where(place > 0, pltpu.roll(gated, 1, 0), 0.0)
    after = jnp.where(place < SEQ - 1, pltpu.roll(gated, gated.shape[0] - 1, 0), 0.0)
    conv = taps[0:1] * before + taps[1:2] * gated + taps[2:3] * after
    mixed[...] = (product(0) * conv).astype(bf)


def mixer(order, own, other, taps, blocks):
    rows = 2 * own.shape[0]
    return pl.pallas_call(
        functools.partial(mixer_kernel, order),
        out_shape=jax.ShapeDtypeStruct((rows, CHANNELS), bf),
        in_specs=[HBM, HBM, VMEM] + [HBM] * 4,
        out_specs=VMEM,
        scratch_shapes=[
            pltpu.VMEM((rows, D), bf),
            whole_scratch(3 * CHANNELS),
            pltpu.SemaphoreType.DMA((18,)),
        ],
        compiler_params=limit(16),
        cost_estimate=pl.CostEstimate(
            flops=2 * rows * D * 3 * CHANNELS, bytes_accessed=8_000_000, transcendentals=0
        ),
    )(own, other, taps, *blocks)


def projected(left, whole, own, other, more=None):
    half = own.shape[0]

    def step(j, _):
        rows = whole[j >> 2, j & 3].reshape(256, whole.shape[-1])
        cols = pl.ds(pl.multiple_of(j * 256, 256), 256)
        sums = dot_t(left[...], rows)
        ours, theirs = sums[:half], sums[half:]
        if more is not None:
            ours, theirs = ours + more[0][:, cols], theirs + more[1][:, cols]
        own[:, cols] = ours.astype(own.dtype)
        other[:, cols] = theirs.astype(other.dtype)
        return 0

    lax.fori_loop(0, 8, step, 0)


def mix_out_kernel(*refs):
    mixed, blocks = refs[:3], refs[3:15]
    own, other, left, whole, sems = refs[15:]
    copies = []
    for c, order in enumerate(ORDERS):
        at = c * CHANNELS
        part = blocks[4 * c : 4 * c + 4]
        copies += fill(order, part, 3 * CHANNELS, CHANNELS, whole, at, sems, len(copies))
        left[:, at : at + CHANNELS] = mixed[c][...]
    finish(copies)
    projected(left, whole, own, other)


def mix_out_product(mixed, blocks):
    rows = mixed[0].shape[0]
    return pl.pallas_call(
        mix_out_kernel,
        out_shape=[
            jax.ShapeDtypeStruct((rows // 2, D), jnp.float32),
            jax.ShapeDtypeStruct((rows // 2, D), bf),
        ],
        in_specs=[VMEM] * 3 + [HBM] * 12,
        out_specs=[VMEM] * 2,
        scratch_shapes=[
            pltpu.VMEM((rows, 3 * CHANNELS), bf),
            whole_scratch(3 * CHANNELS),
            pltpu.SemaphoreType.DMA((36,)),
        ],
        compiler_params=limit(16),
        cost_estimate=pl.CostEstimate(
            flops=2 * rows * D * 3 * CHANNELS, bytes_accessed=9_000_000, transcendentals=0
        ),
    )(*mixed, *blocks)


def feed_kernel(stage, first_own, first_other, *refs):
    blocks, refs = refs[:12], refs[12:]
    more, sums = refs[:2], refs[9:]
    own, other, x, up, down, hidden, sems = refs[2:9] if stage else refs
    tokens = both_tokens(first_own, first_other, x, sems, 0)
    used = 2
    ups, downs = [], []
    for whole, table, sets in ((up, UPS, ups), (down, DOWNS, downs)):
        for c, order in enumerate(ORDERS):
            n = table[stage][c]
            ring = blocks[4 * c : 4 * c + 4]
            start = UPS[stage][c] if sets is downs else 0
            shift = stage * (UPS[0][c] + DOWNS[0][c])
            at = sum(table[stage][:c])
            sets.append(fill(order, ring, start, n, whole, at, sems, used, shift))
            used += len(sets[-1])
    if stage:
        for src, dst in zip(more, sums):
            downs.append([pltpu.make_async_copy(src, dst, sems.at[used])])
            used += 1
    for copy in sum(ups + downs, tokens):
        copy.start()
    for copy in tokens:
        copy.wait()

    def step(j, _):
        cols = pl.ds(pl.multiple_of(j * 256, 256), 256)
        raised = jnp.maximum(dot(x[...], up[..., cols].reshape(D, 256)), 0.0)
        hidden[:, cols] = (raised * raised).astype(bf)
        return 0

    done = 0
    for c, copies in enumerate(ups):
        for copy in copies:
            copy.wait()
        ready = sum(UPS[stage][: c + 1]) // 256
        lax.fori_loop(done, ready, step, 0)
        done = ready
    for copy in sum(downs, []):
        copy.wait()
    projected(hidden, down, own, other, sums if stage else None)


def feed(stage, own, other, blocks, more=None):
    half = own.shape[0]
    width = HIDDEN
    extra = [] if more is None else list(more)
    last = jnp.float32 if more is None else bf
    return pl.pallas_call(
        functools.partial(feed_kernel, stage),
        out_shape=[
            jax.ShapeDtypeStruct((half, D), jnp.float32),
            jax.ShapeDtypeStruct((half, D), last),
        ],
        in_specs=[HBM] * (2 + len(blocks) + len(extra)),
        out_specs=[VMEM] * 2,
        scratch_shapes=[
            pltpu.VMEM((2 * half, D), bf),
            whole_scratch(width),
            whole_scratch(width),
            pltpu.VMEM((2 * half, width), bf),
            pltpu.SemaphoreType.DMA((80,)),
        ]
        + [pltpu.VMEM((half, D), jnp.float32) for _ in extra],
        compiler_params=limit(21 + 5 * stage),
        cost_estimate=pl.CostEstimate(
            flops=8 * half * D * width, bytes_accessed=20_000_000, transcendentals=0
        ),
    )(own, other, *blocks, *extra)


def joined_kernel(skip, own, other, gain, out):
    def step(i, _):
        rows = pl.ds(pl.multiple_of(i * 128, 128), 128)
        values = residual_scale * skip[rows].astype(jnp.float32)
        values = values + (own[rows] + other[rows].astype(jnp.float32))
        center = values - jnp.mean(values, axis=-1, keepdims=True)
        spread = jnp.mean(center * center, axis=-1, keepdims=True)
        out[rows] = (center * lax.rsqrt(spread + norm_epsilon) * gain[...]).astype(bf)
        return 0

    lax.fori_loop(0, out.shape[0] // 128, step, 0)


def joined(skip, own, other, gain):
    other = swapped(other)
    return pl.pallas_call(
        joined_kernel,
        out_shape=jax.ShapeDtypeStruct(skip.shape, bf),
        in_specs=[VMEM] * 4,
        out_specs=VMEM,
        compiler_params=limit(16),
    )(skip, own, other, gain.reshape(1, -1))


def local(
    tokens,
    outer_weight,
    inner_weight,
    value_weight,
    conv_taps,
    mix_out,
    norm_first,
    up_weight,
    down_weight,
    norm_second,
):
    parts = pieces(outer_weight, inner_weight, value_weight, mix_out.T, up_weight, down_weight.T)
    tokens_other = swapped(tokens)
    near = []
    for c, order in enumerate(ORDERS):
        ring = around(parts[c], order[0])
        near += placed(ring, order[0], [(0, parts[c].shape[-1])])
    blocks = [[], [], []]
    for c, order in enumerate(ORDERS):
        ring = around(near[c], order[1])
        head, one, two = stage_widths(c)
        (own,) = placed(ring, order[1], [(0, head)])
        columns = [(head, one), (head + one, two), (head, one + two)]
        *own_stages, own_both = placed(ring, order[1], columns)
        blocks[0] += around(own, order[2])
        back = moved(own_both, order[2], 3)
        for s, own in enumerate(own_stages, 1):
            ahead = moved(own, order[2], 1)
            blocks[s] += [own, ahead, moved(ahead, order[2], 1), back]

    mixed = []
    for c, order in enumerate(ORDERS):
        taps = conv_taps[:, c * CHANNELS : (c + 1) * CHANNELS]
        mixed.append(mixer(order, tokens, tokens_other, taps, blocks[0][4 * c : 4 * c + 4]))
    own, other = mix_out_product(mixed, blocks[0])
    first = joined(tokens, own, other, norm_first)
    first_other = swapped(first)
    sums = feed(0, first, first_other, blocks[1])
    own, other = feed(1, first, first_other, blocks[2], sums)
    return joined(first, own, other, norm_second)


def solution(mesh):
    finer = Mesh(
        mesh.devices.reshape(2, 2, 4, 4, 2),
        ("rep", "fs_0", "fs_1", "fs_2", "tp"),
    )
    placement = (
        P(REP_FS_TP, None),
        P(FS, "tp"),
        P(FS, "tp"),
        P(FS, "tp"),
        P(None, "tp"),
        P("tp", FS),
        P(),
        P(FS, "tp"),
        P("tp", FS),
        P(),
    )
    return jax.shard_map(
        local, mesh=finer, in_specs=placement, out_specs=P(REP_FS_TP, None), check_vma=False
    )
```

```python
import functools

import jax
import jax.numpy as jnp
from jax import lax
from jax.experimental import pallas as pl
from jax.experimental.pallas import tpu as pltpu
from jax.sharding import Mesh
from jax.sharding import PartitionSpec as P


SEQ = 128
D = 2048
ROWS = 32
FS = ("fs_0", "fs_1", "fs_2")
REP_FS_TP = ("rep", "fs_0", "fs_1", "fs_2", "tp")
ORDERS = ("zxy", "xyz", "yzx")
CHANNELS = 256
HIDDEN = 1024
UPS = ((384, 384, 256), (384, 384, 256))
DOWNS = ((256, 384, 384), (384, 256, 384))


residual_scale = 2.0**0.25
norm_epsilon = 1e-05
bf = jnp.bfloat16
HBM = pl.BlockSpec(memory_space=pltpu.HBM)
VMEM = pl.BlockSpec(memory_space=pltpu.VMEM)


def limit(mebibytes):
    return pltpu.CompilerParams(vmem_limit_bytes=mebibytes * 1024 * 1024)


def in_hbm(arrays):
    return [pltpu.with_memory_space_constraint(a, pltpu.HBM) for a in arrays]


def stage_widths(part):
    return [4 * CHANNELS] + [UPS[s][part] + DOWNS[s][part] for s in range(2)]


def position(axis):
    if axis == "z":
        return lax.axis_index("rep") * 2 + lax.axis_index("fs_0")
    return lax.axis_index({"y": "fs_1", "x": "fs_2"}[axis])


def source(axis, step):
    way = 2 * lax.axis_index("tp") - 1
    return (position(axis) + 4 + way * step) & 3


def ring_pairs(axis, step):
    at = "zyx".index(axis)
    pairs = []
    for z in range(4):
        for y in range(4):
            for x in range(4):
                for core in range(2):
                    to = [z, y, x]
                    to[at] = (to[at] + (step if core == 0 else 4 - step)) % 4
                    start = ((z * 4 + y) * 4 + x) * 2 + core
                    pairs.append((start, ((to[0] * 4 + to[1]) * 4 + to[2]) * 2 + core))
    return pairs


def moved(block, axis, step):
    return lax.ppermute(block, REP_FS_TP, ring_pairs(axis, step))


def around(block, axis):
    near, back = moved(block, axis, 1), moved(block, axis, 3)
    return [block, near, moved(near, axis, 1), back]


def swapped(x):
    return lax.ppermute(x, "tp", [(0, 1), (1, 0)])


def finish(copies):
    for copy in copies:
        copy.start()
    for copy in copies:
        copy.wait()


def pieces_kernel(*refs):
    weights, outs, held, sems = refs[:6], refs[6:9], refs[9:15], refs[15]
    rows = pl.ds(lax.axis_index("rep") * ROWS, ROWS)
    finish(
        [
            pltpu.make_async_copy(w.at[rows], h, sems.at[i])
            for i, (w, h) in enumerate(zip(weights, held))
        ]
    )
    outer, inner, value, mix, up, down = held
    for part, out in enumerate(outs):
        at = 0
        for w in (outer, inner, value, mix):
            out[:, at : at + CHANNELS] = w[:, part * CHANNELS : (part + 1) * CHANNELS].astype(bf)
            at += CHANNELS
        for s in range(2):
            for w, shares in ((up, UPS[s]), (down, DOWNS[s])):
                start, n = s * HIDDEN + sum(shares[:part]), shares[part]
                out[:, at : at + n] = w[:, start : start + n].astype(bf)
                at += n


def pieces(*weights):
    return pl.pallas_call(
        pieces_kernel,
        out_shape=[jax.ShapeDtypeStruct((ROWS, sum(stage_widths(c))), bf) for c in range(3)],
        in_specs=[HBM] * 6,
        out_specs=[VMEM] * 3,
        scratch_shapes=[pltpu.VMEM((ROWS, w.shape[1]), jnp.float32) for w in weights]
        + [pltpu.SemaphoreType.DMA((6,))],
        compiler_params=limit(6),
    )(*in_hbm(weights))


def place_kernel(axis, columns, *refs):
    parts, outs, sems = refs[:4], refs[4:-1], refs[-1]
    copies = []
    for k, part in enumerate(parts):
        for (start, width), out in zip(columns, outs):
            src, dst = part.at[..., pl.ds(start, width)], out.at[source(axis, k)]
            copies.append(pltpu.make_async_copy(src, dst, sems.at[len(copies)]))
    finish(copies)


def placed(parts, axis, columns, space):
    lead = parts[0].shape[:-1]
    return pl.pallas_call(
        functools.partial(place_kernel, axis, columns),
        out_shape=[space((4, *lead, width), bf) for _, width in columns],
        in_specs=[HBM] * 4,
        out_specs=[pl.BlockSpec(memory_space=space)] * len(columns),
        scratch_shapes=[pltpu.SemaphoreType.DMA((4 * len(columns),))],
        compiler_params=limit(4),
    )(*parts)


def fill(order, blocks, start, width, whole, at, sems, used, shift=0):
    copies = []

    def add(src, dst):
        copies.append(pltpu.make_async_copy(src, dst, sems.at[used + len(copies)]))

    cd = pl.ds(at, width)
    for k, block in enumerate(blocks):
        p = source(order[2], k)
        cs = pl.ds(start + (shift if k == 3 else 0), width)
        if order == "xyz":
            add(block.at[:, :, :, cs], whole.at[p & 1, :, :, p >> 1, :, cd])
        else:
            for z in range(4):
                if order == "zxy":
                    add(block.at[:, z, :, cs], whole.at[z & 1, p, :, z >> 1, :, cd])
                else:
                    add(block.at[z, :, :, cs], whole.at[z & 1, :, p, z >> 1, :, cd])
    return copies


def whole_scratch(width):
    return pltpu.VMEM((2, 4, 4, 2, ROWS, width), bf)


def dot(a, b):
    return jnp.dot(a, b, preferred_element_type=jnp.float32)


def dot_t(a, b):
    return lax.dot_general(a, b, (((1,), (1,)), ((), ())), preferred_element_type=jnp.float32)


def both_tokens(own, other, x, sems, used):
    half = own.shape[0]
    return [
        pltpu.make_async_copy(own, x.at[pl.ds(0, half)], sems.at[used]),
        pltpu.make_async_copy(other, x.at[pl.ds(half, half)], sems.at[used + 1]),
    ]


def mixer_kernel(order, own, other, taps, *refs):
    blocks, mixed, x, w, sems = refs[:4], refs[4], refs[5], refs[6], refs[7]
    copies = both_tokens(own, other, x, sems, 0)
    copies += fill(order, blocks, 0, 3 * CHANNELS, w, 0, sems, 2)
    finish(copies)

    def product(i):
        return dot(x[...], w[..., i * CHANNELS : (i + 1) * CHANNELS].reshape(D, CHANNELS))

    gated = product(1) * product(2)
    place = lax.broadcasted_iota(jnp.int32, gated.shape, 0) & (SEQ - 1)
    before = jnp.where(place > 0, pltpu.roll(gated, 1, 0), 0.0)
    after = jnp.where(place < SEQ - 1, pltpu.roll(gated, gated.shape[0] - 1, 0), 0.0)
    conv = taps[0:1] * before + taps[1:2] * gated + taps[2:3] * after
    mixed[...] = (product(0) * conv).astype(bf)


def mixer(order, own, other, taps, blocks):
    rows = 2 * own.shape[0]
    return pl.pallas_call(
        functools.partial(mixer_kernel, order),
        out_shape=jax.ShapeDtypeStruct((rows, CHANNELS), bf),
        in_specs=[HBM, HBM, VMEM] + [HBM] * 4,
        out_specs=VMEM,
        scratch_shapes=[
            pltpu.VMEM((rows, D), bf),
            whole_scratch(3 * CHANNELS),
            pltpu.SemaphoreType.DMA((18,)),
        ],
        compiler_params=limit(16),
        cost_estimate=pl.CostEstimate(
            flops=2 * rows * D * 3 * CHANNELS, bytes_accessed=8_000_000, transcendentals=0
        ),
    )(own, other, taps, *blocks)


def projected(lefts, whole, outs, more=None):
    def step(j, _):
        rows = whole[j >> 2, j & 3].reshape(256, whole.shape[-1])
        cols = pl.ds(pl.multiple_of(j * 256, 256), 256)
        for left, parts in zip(lefts, outs):
            sums = dot_t(left[...], rows)
            if more is not None:
                sums = sums + more[:, cols]
            size = sums.shape[0] // len(parts)
            for i, out in enumerate(parts):
                out[:, cols] = sums[i * size : (i + 1) * size].astype(out.dtype)
        return 0

    lax.fori_loop(0, 8, step, 0)


def mix_out_kernel(*refs):
    mixed, blocks = refs[:3], refs[3:15]
    own, other, left, whole, sems = refs[15:]
    copies = []
    for c, order in enumerate(ORDERS):
        at = c * CHANNELS
        part = blocks[4 * c : 4 * c + 4]
        copies += fill(order, part, 3 * CHANNELS, CHANNELS, whole, at, sems, len(copies))
        left[:, at : at + CHANNELS] = mixed[c][...]
    finish(copies)
    projected([left], whole, [(own, other)])


def mix_out_product(mixed, blocks):
    rows = mixed[0].shape[0]
    return pl.pallas_call(
        mix_out_kernel,
        out_shape=[
            pltpu.VMEM((rows // 2, D), jnp.float32),
            pltpu.VMEM((rows // 2, D), bf),
        ],
        in_specs=[VMEM] * 3 + [HBM] * 12,
        out_specs=[VMEM] * 2,
        scratch_shapes=[
            pltpu.VMEM((rows, 3 * CHANNELS), bf),
            whole_scratch(3 * CHANNELS),
            pltpu.SemaphoreType.DMA((36,)),
        ],
        compiler_params=limit(16),
        cost_estimate=pl.CostEstimate(
            flops=2 * rows * D * 3 * CHANNELS, bytes_accessed=9_000_000, transcendentals=0
        ),
    )(*mixed, *blocks)


def feed_kernel(stage, first_own, first_other, *refs):
    blocks, refs = refs[:12], refs[12:]
    half = first_own.shape[0]
    if stage:
        more, other, hidden_own, down, x, up, hidden, sems, sums = refs
    else:
        own, other, x, up, down, hidden, sems = refs
    tokens = both_tokens(first_own, first_other, x, sems, 0)
    used = 2
    ups, downs = [], []
    for whole, table, sets in ((up, UPS, ups), (down, DOWNS, downs)):
        for c, order in enumerate(ORDERS):
            n = table[stage][c]
            ring = blocks[4 * c : 4 * c + 4]
            start = UPS[stage][c] if sets is downs else 0
            shift = stage * (UPS[0][c] + DOWNS[0][c])
            at = sum(table[stage][:c])
            sets.append(fill(order, ring, start, n, whole, at, sems, used, shift))
            used += len(sets[-1])
    if stage:
        downs.append([pltpu.make_async_copy(more, sums, sems.at[used])])
    for copy in sum(ups + downs, tokens):
        copy.start()
    for copy in tokens:
        copy.wait()

    def step(j, _):
        cols = pl.ds(pl.multiple_of(j * 256, 256), 256)
        raised = jnp.maximum(dot(x[...], up[..., cols].reshape(D, 256)), 0.0)
        squared = (raised * raised).astype(bf)
        if stage:
            hidden_own[:, cols] = squared[:half]
            hidden[:, cols] = squared[half:]
        else:
            hidden[:, cols] = squared
        return 0

    done = 0
    for c, copies in enumerate(ups):
        for copy in copies:
            copy.wait()
        ready = sum(UPS[stage][: c + 1]) // 256
        lax.fori_loop(done, ready, step, 0)
        done = ready
    for copy in sum(downs, []):
        copy.wait()
    if stage:
        projected([hidden], down, [(other,)], sums)
    else:
        projected([hidden], down, [(own, other)])


def feed(stage, own, other, blocks, more=None):
    half = own.shape[0]
    down = (2, 4, 4, 2, ROWS, HIDDEN)
    sums = pltpu.VMEM((half, D), jnp.float32)
    if stage:
        outs = [pltpu.VMEM((half, D), bf), pltpu.VMEM((half, HIDDEN), bf), pltpu.VMEM(down, bf)]
        scratch = [pltpu.VMEM((half, HIDDEN), bf), pltpu.SemaphoreType.DMA((80,)), sums]
        inputs = (*blocks, more)
    else:
        outs = [sums, sums]
        scratch = [
            whole_scratch(HIDDEN),
            pltpu.VMEM((2 * half, HIDDEN), bf),
            pltpu.SemaphoreType.DMA((80,)),
        ]
        inputs = blocks
    return pl.pallas_call(
        functools.partial(feed_kernel, stage),
        out_shape=outs,
        in_specs=[HBM] * (2 + len(inputs)),
        out_specs=[VMEM] * len(outs),
        scratch_shapes=[pltpu.VMEM((2 * half, D), bf), whole_scratch(HIDDEN)] + scratch,
        compiler_params=limit(21),
        cost_estimate=pl.CostEstimate(
            flops=(6 if stage else 8) * half * D * HIDDEN,
            bytes_accessed=20_000_000,
            transcendentals=0,
        ),
    )(own, other, *inputs)


def finished_kernel(hidden, down, more, own):
    projected([hidden], down, [(own,)], more)


def finished(hidden, down, more):
    half = hidden.shape[0]
    return pl.pallas_call(
        finished_kernel,
        out_shape=pltpu.VMEM((half, D), jnp.float32),
        in_specs=[VMEM] * 3,
        out_specs=VMEM,
        compiler_params=limit(18),
        cost_estimate=pl.CostEstimate(
            flops=2 * half * D * HIDDEN, bytes_accessed=10_000_000, transcendentals=0
        ),
    )(hidden, down, more)


def joined_kernel(skip, own, other, gain, out):
    def step(i, _):
        rows = pl.ds(pl.multiple_of(i * 128, 128), 128)
        values = residual_scale * skip[rows].astype(jnp.float32)
        values = values + (own[rows] + other[rows].astype(jnp.float32))
        center = values - jnp.mean(values, axis=-1, keepdims=True)
        spread = jnp.mean(center * center, axis=-1, keepdims=True)
        out[rows] = (center * lax.rsqrt(spread + norm_epsilon) * gain[...]).astype(bf)
        return 0

    lax.fori_loop(0, out.shape[0] // 128, step, 0)


def joined(skip, own, other, gain):
    return pl.pallas_call(
        joined_kernel,
        out_shape=jax.ShapeDtypeStruct(skip.shape, bf),
        in_specs=[VMEM] * 4,
        out_specs=VMEM,
        compiler_params=limit(16),
    )(skip, own, other, gain.reshape(1, -1))


def local(
    tokens,
    outer_weight,
    inner_weight,
    value_weight,
    conv_taps,
    mix_out,
    norm_first,
    up_weight,
    down_weight,
    norm_second,
):
    parts = pieces(outer_weight, inner_weight, value_weight, mix_out.T, up_weight, down_weight.T)
    tokens_other = swapped(tokens)
    near = []
    for c, order in enumerate(ORDERS):
        ring = around(parts[c], order[0])
        near += placed(ring, order[0], [(0, parts[c].shape[-1])], pltpu.VMEM)
    blocks = [[], [], []]
    for c, order in enumerate(ORDERS):
        ring = around(near[c], order[1])
        head, one, two = stage_widths(c)
        (own,) = placed(ring, order[1], [(0, head)], pltpu.VMEM)
        columns = [(head, one), (head + one, two), (head, one + two)]
        *own_stages, own_both = placed(ring, order[1], columns, pltpu.HBM)
        blocks[0] += around(own, order[2])
        back = moved(own_both, order[2], 3)
        for s, own in enumerate(own_stages, 1):
            ahead = moved(own, order[2], 1)
            blocks[s] += [own, ahead, moved(ahead, order[2], 1), back]

    mixed = []
    for c, order in enumerate(ORDERS):
        taps = conv_taps[:, c * CHANNELS : (c + 1) * CHANNELS]
        mixed.append(mixer(order, tokens, tokens_other, taps, blocks[0][4 * c : 4 * c + 4]))
    own, other = mix_out_product(mixed, blocks[0])
    other = swapped(other)
    first = joined(tokens, own, other, norm_first)
    first_other = swapped(first)
    own, other = feed(0, first, first_other, blocks[1])
    other, hidden, down = feed(1, first, first_other, blocks[2], other)
    other = swapped(other)
    own = finished(hidden, down, own)
    return joined(first, own, other, norm_second)


def solution(mesh):
    finer = Mesh(
        mesh.devices.reshape(2, 2, 4, 4, 2),
        ("rep", "fs_0", "fs_1", "fs_2", "tp"),
    )
    placement = (
        P(REP_FS_TP, None),
        P(FS, "tp"),
        P(FS, "tp"),
        P(FS, "tp"),
        P(None, "tp"),
        P("tp", FS),
        P(),
        P(FS, "tp"),
        P("tp", FS),
        P(),
    )
    return jax.shard_map(
        local, mesh=finer, in_specs=placement, out_specs=P(REP_FS_TP, None), check_vma=False
    )
```

```python
import functools

import jax
import jax.numpy as jnp
from jax import lax
from jax.experimental import pallas as pl
from jax.experimental.pallas import tpu as pltpu
from jax.sharding import Mesh
from jax.sharding import PartitionSpec as P


SEQ = 128
D = 2048
ROWS = 32
FS = ("fs_0", "fs_1", "fs_2")
REP_FS_TP = ("rep", "fs_0", "fs_1", "fs_2", "tp")
ORDERS = ("zxy", "xyz", "yzx")
CHANNELS = 256
HIDDEN = 1024
UPS = ((384, 384, 256), (384, 384, 256))
DOWNS = ((256, 384, 384), (384, 256, 384))


residual_scale = 2.0**0.25
norm_epsilon = 1e-05
bf = jnp.bfloat16
HBM = pl.BlockSpec(memory_space=pltpu.HBM)
VMEM = pl.BlockSpec(memory_space=pltpu.VMEM)


def limit(mebibytes):
    return pltpu.CompilerParams(vmem_limit_bytes=mebibytes * 1024 * 1024)


def in_hbm(arrays):
    return [pltpu.with_memory_space_constraint(a, pltpu.HBM) for a in arrays]


def stage_widths(part):
    return [4 * CHANNELS] + [UPS[s][part] + DOWNS[s][part] for s in range(2)]


def position(axis):
    if axis == "z":
        return lax.axis_index("rep") * 2 + lax.axis_index("fs_0")
    return lax.axis_index({"y": "fs_1", "x": "fs_2"}[axis])


def source(axis, step):
    way = 2 * lax.axis_index("tp") - 1
    return (position(axis) + 4 + way * step) & 3


def ring_pairs(axis, step):
    at = "zyx".index(axis)
    pairs = []
    for z in range(4):
        for y in range(4):
            for x in range(4):
                for core in range(2):
                    to = [z, y, x]
                    to[at] = (to[at] + (step if core == 0 else 4 - step)) % 4
                    start = ((z * 4 + y) * 4 + x) * 2 + core
                    pairs.append((start, ((to[0] * 4 + to[1]) * 4 + to[2]) * 2 + core))
    return pairs


def moved(block, axis, step):
    return lax.ppermute(block, REP_FS_TP, ring_pairs(axis, step))


def around(block, axis):
    near, back = moved(block, axis, 1), moved(block, axis, 3)
    return [block, near, moved(near, axis, 1), back]


def swapped(x):
    return lax.ppermute(x, "tp", [(0, 1), (1, 0)])


def finish(copies):
    for copy in copies:
        copy.start()
    for copy in copies:
        copy.wait()


def pieces_kernel(*refs):
    weights, outs, held, sems = refs[:6], refs[6:9], refs[9:15], refs[15]
    rows = pl.ds(lax.axis_index("rep") * ROWS, ROWS)
    finish(
        [
            pltpu.make_async_copy(w.at[rows], h, sems.at[i])
            for i, (w, h) in enumerate(zip(weights, held))
        ]
    )
    outer, inner, value, mix, up, down = held
    for part, out in enumerate(outs):
        at = 0
        for w in (outer, inner, value, mix):
            out[:, at : at + CHANNELS] = w[:, part * CHANNELS : (part + 1) * CHANNELS].astype(bf)
            at += CHANNELS
        for s in range(2):
            for w, shares in ((up, UPS[s]), (down, DOWNS[s])):
                start, n = s * HIDDEN + sum(shares[:part]), shares[part]
                out[:, at : at + n] = w[:, start : start + n].astype(bf)
                at += n


def pieces(*weights):
    return pl.pallas_call(
        pieces_kernel,
        out_shape=[jax.ShapeDtypeStruct((ROWS, sum(stage_widths(c))), bf) for c in range(3)],
        in_specs=[HBM] * 6,
        out_specs=[VMEM] * 3,
        scratch_shapes=[pltpu.VMEM((ROWS, w.shape[1]), jnp.float32) for w in weights]
        + [pltpu.SemaphoreType.DMA((6,))],
        compiler_params=limit(6),
    )(*in_hbm(weights))


def place_kernel(axis, columns, *refs):
    parts, outs, sems = refs[:4], refs[4:-1], refs[-1]
    copies = []
    for k, part in enumerate(parts):
        for (start, width), out in zip(columns, outs):
            src, dst = part.at[..., pl.ds(start, width)], out.at[source(axis, k)]
            copies.append(pltpu.make_async_copy(src, dst, sems.at[len(copies)]))
    finish(copies)


def placed(parts, axis, columns, space):
    lead = parts[0].shape[:-1]
    return pl.pallas_call(
        functools.partial(place_kernel, axis, columns),
        out_shape=[space((4, *lead, width), bf) for _, width in columns],
        in_specs=[HBM] * 4,
        out_specs=[pl.BlockSpec(memory_space=space)] * len(columns),
        scratch_shapes=[pltpu.SemaphoreType.DMA((4 * len(columns),))],
        compiler_params=limit(4),
    )(*parts)


def fill(order, blocks, start, width, whole, at, sems, used, shift=0):
    copies = []

    def add(src, dst):
        copies.append(pltpu.make_async_copy(src, dst, sems.at[used + len(copies)]))

    cd = pl.ds(at, width)
    for k, block in enumerate(blocks):
        p = source(order[2], k)
        cs = pl.ds(start + (shift if k == 3 else 0), width)
        if order == "xyz":
            add(block.at[:, :, :, cs], whole.at[p & 1, :, :, p >> 1, :, cd])
        else:
            for z in range(4):
                if order == "zxy":
                    add(block.at[:, z, :, cs], whole.at[z & 1, p, :, z >> 1, :, cd])
                else:
                    add(block.at[z, :, :, cs], whole.at[z & 1, :, p, z >> 1, :, cd])
    return copies


def whole_scratch(width):
    return pltpu.VMEM((2, 4, 4, 2, ROWS, width), bf)


def dot(a, b):
    return jnp.dot(a, b, preferred_element_type=jnp.float32)


def dot_t(a, b):
    return lax.dot_general(a, b, (((1,), (1,)), ((), ())), preferred_element_type=jnp.float32)


def both_tokens(own, other, x, sems, used):
    half = own.shape[0]
    return [
        pltpu.make_async_copy(own, x.at[pl.ds(0, half)], sems.at[used]),
        pltpu.make_async_copy(other, x.at[pl.ds(half, half)], sems.at[used + 1]),
    ]


def mixer_kernel(order, own, other, taps, *refs):
    blocks, mixed, x, w, sems = refs[:4], refs[4], refs[5], refs[6], refs[7]
    copies = both_tokens(own, other, x, sems, 0)
    copies += fill(order, blocks, 0, 3 * CHANNELS, w, 0, sems, 2)
    finish(copies)

    def product(i):
        return dot(x[...], w[..., i * CHANNELS : (i + 1) * CHANNELS].reshape(D, CHANNELS))

    gated = product(1) * product(2)
    place = lax.broadcasted_iota(jnp.int32, gated.shape, 0) & (SEQ - 1)
    before = jnp.where(place > 0, pltpu.roll(gated, 1, 0), 0.0)
    after = jnp.where(place < SEQ - 1, pltpu.roll(gated, gated.shape[0] - 1, 0), 0.0)
    conv = taps[0:1] * before + taps[1:2] * gated + taps[2:3] * after
    mixed[...] = (product(0) * conv).astype(bf)


def mixer(order, own, other, taps, blocks):
    rows = 2 * own.shape[0]
    return pl.pallas_call(
        functools.partial(mixer_kernel, order),
        out_shape=jax.ShapeDtypeStruct((rows, CHANNELS), bf),
        in_specs=[HBM, HBM, VMEM] + [HBM] * 4,
        out_specs=VMEM,
        scratch_shapes=[
            pltpu.VMEM((rows, D), bf),
            whole_scratch(3 * CHANNELS),
            pltpu.SemaphoreType.DMA((18,)),
        ],
        compiler_params=limit(16),
        cost_estimate=pl.CostEstimate(
            flops=2 * rows * D * 3 * CHANNELS, bytes_accessed=8_000_000, transcendentals=0
        ),
    )(own, other, taps, *blocks)


def projected(lefts, whole, outs, more=None):
    def step(j, _):
        rows = whole[j >> 2, j & 3].reshape(256, whole.shape[-1])
        cols = pl.ds(pl.multiple_of(j * 256, 256), 256)
        for left, parts in zip(lefts, outs):
            sums = dot_t(left[...], rows)
            if more is not None:
                sums = sums + more[:, cols]
            size = sums.shape[0] // len(parts)
            for i, out in enumerate(parts):
                out[:, cols] = sums[i * size : (i + 1) * size].astype(out.dtype)
        return 0

    lax.fori_loop(0, 8, step, 0)


def mix_out_kernel(*refs):
    mixed, blocks = refs[:3], refs[3:15]
    own, other, left, whole, sems = refs[15:]
    copies = []
    for c, order in enumerate(ORDERS):
        at = c * CHANNELS
        part = blocks[4 * c : 4 * c + 4]
        copies += fill(order, part, 3 * CHANNELS, CHANNELS, whole, at, sems, len(copies))
        left[:, at : at + CHANNELS] = mixed[c][...]
    finish(copies)
    projected([left], whole, [(own, other)])


def mix_out_product(mixed, blocks):
    rows = mixed[0].shape[0]
    return pl.pallas_call(
        mix_out_kernel,
        out_shape=[
            pltpu.VMEM((rows // 2, D), jnp.float32),
            pltpu.VMEM((rows // 2, D), bf),
        ],
        in_specs=[VMEM] * 3 + [HBM] * 12,
        out_specs=[VMEM] * 2,
        scratch_shapes=[
            pltpu.VMEM((rows, 3 * CHANNELS), bf),
            whole_scratch(3 * CHANNELS),
            pltpu.SemaphoreType.DMA((36,)),
        ],
        compiler_params=limit(16),
        cost_estimate=pl.CostEstimate(
            flops=2 * rows * D * 3 * CHANNELS, bytes_accessed=9_000_000, transcendentals=0
        ),
    )(*mixed, *blocks)


def feed_kernel(stage, first_own, first_other, *refs):
    blocks, refs = refs[:12], refs[12:]
    half = first_own.shape[0]
    if stage:
        more, other, hidden_own, down, x, up, hidden, sems, sums = refs
    else:
        own, other, x, up, down, hidden, sems = refs
    tokens = both_tokens(first_own, first_other, x, sems, 0)
    used = 2
    ups, downs = [], []
    for whole, table, sets in ((up, UPS, ups), (down, DOWNS, downs)):
        for c, order in enumerate(ORDERS):
            n = table[stage][c]
            ring = blocks[4 * c : 4 * c + 4]
            start = UPS[stage][c] if sets is downs else 0
            shift = stage * (UPS[0][c] + DOWNS[0][c])
            at = sum(table[stage][:c])
            sets.append(fill(order, ring, start, n, whole, at, sems, used, shift))
            used += len(sets[-1])
    if stage:
        downs.append([pltpu.make_async_copy(more, sums, sems.at[used])])
    for copy in sum(ups + downs, tokens):
        copy.start()
    for copy in tokens:
        copy.wait()

    def step(j, _):
        cols = pl.ds(pl.multiple_of(j * 256, 256), 256)
        raised = jnp.maximum(dot(x[...], up[..., cols].reshape(D, 256)), 0.0)
        squared = (raised * raised).astype(bf)
        if stage:
            hidden_own[:, cols] = squared[:half]
            hidden[:, cols] = squared[half:]
        else:
            hidden[:, cols] = squared
        return 0

    done = 0
    for c, copies in enumerate(ups):
        for copy in copies:
            copy.wait()
        ready = sum(UPS[stage][: c + 1]) // 256
        lax.fori_loop(done, ready, step, 0)
        done = ready
    for copy in sum(downs, []):
        copy.wait()
    if stage:
        projected([hidden], down, [(other,)], sums)
    else:
        projected([hidden], down, [(own, other)])


def feed(stage, own, other, blocks, more=None):
    half = own.shape[0]
    down = (2, 4, 4, 2, ROWS, HIDDEN)
    sums = pltpu.VMEM((half, D), jnp.float32)
    if stage:
        outs = [pltpu.VMEM((half, D), bf), pltpu.VMEM((half, HIDDEN), bf), pltpu.VMEM(down, bf)]
        scratch = [pltpu.VMEM((half, HIDDEN), bf), pltpu.SemaphoreType.DMA((80,)), sums]
        inputs = (*blocks, more)
    else:
        outs = [sums, sums]
        scratch = [
            whole_scratch(HIDDEN),
            pltpu.VMEM((2 * half, HIDDEN), bf),
            pltpu.SemaphoreType.DMA((80,)),
        ]
        inputs = blocks
    return pl.pallas_call(
        functools.partial(feed_kernel, stage),
        out_shape=outs,
        in_specs=[HBM] * (2 + len(inputs)),
        out_specs=[VMEM] * len(outs),
        scratch_shapes=[pltpu.VMEM((2 * half, D), bf), whole_scratch(HIDDEN)] + scratch,
        compiler_params=limit(21),
        cost_estimate=pl.CostEstimate(
            flops=(6 if stage else 8) * half * D * HIDDEN,
            bytes_accessed=20_000_000,
            transcendentals=0,
        ),
    )(own, other, *inputs)


def finished_kernel(hidden, down, more, own):
    projected([hidden], down, [(own,)], more)


def finished(hidden, down, more):
    half = hidden.shape[0]
    return pl.pallas_call(
        finished_kernel,
        out_shape=pltpu.VMEM((half, D), jnp.float32),
        in_specs=[VMEM] * 3,
        out_specs=VMEM,
        compiler_params=limit(18),
        cost_estimate=pl.CostEstimate(
            flops=2 * half * D * HIDDEN, bytes_accessed=10_000_000, transcendentals=0
        ),
    )(hidden, down, more)


def joined_kernel(skip, own, other, gain, out, *scratch):
    size = out.shape[0] // 3

    def leaving(i, rows):
        held, sems = scratch
        return pltpu.make_async_copy(held.at[rows], out.at[rows], sems.at[i])

    def step(i, _):
        rows = pl.ds(pl.multiple_of(i * size, size), size)
        values = residual_scale * skip[rows].astype(jnp.float32)
        values = values + (own[rows] + other[rows].astype(jnp.float32))
        center = values - jnp.mean(values, axis=-1, keepdims=True)
        spread = jnp.mean(center * center, axis=-1, keepdims=True)
        normed = (center * lax.rsqrt(spread + norm_epsilon) * gain[...]).astype(bf)
        if scratch:
            scratch[0][rows] = normed
            leaving(i, rows).start()
        else:
            out[rows] = normed
        return 0

    lax.fori_loop(0, 3, step, 0)
    if scratch:
        for i in range(3):
            leaving(i, pl.ds(i * size, size)).wait()


def joined(skip, own, other, gain, last):
    scratch = [pltpu.VMEM(skip.shape, bf), pltpu.SemaphoreType.DMA((3,))]
    return pl.pallas_call(
        joined_kernel,
        out_shape=jax.ShapeDtypeStruct(skip.shape, bf),
        in_specs=[VMEM] * 4,
        out_specs=HBM if last else VMEM,
        scratch_shapes=scratch if last else [],
        compiler_params=limit(16),
    )(skip, own, other, gain.reshape(1, -1))


def local(
    tokens,
    outer_weight,
    inner_weight,
    value_weight,
    conv_taps,
    mix_out,
    norm_first,
    up_weight,
    down_weight,
    norm_second,
):
    parts = pieces(outer_weight, inner_weight, value_weight, mix_out.T, up_weight, down_weight.T)
    tokens_other = swapped(tokens)
    near = []
    for c, order in enumerate(ORDERS):
        ring = around(parts[c], order[0])
        near += placed(ring, order[0], [(0, parts[c].shape[-1])], pltpu.VMEM)
    blocks = [[], [], []]
    for c, order in enumerate(ORDERS):
        ring = around(near[c], order[1])
        head, one, two = stage_widths(c)
        (own,) = placed(ring, order[1], [(0, head)], pltpu.VMEM)
        columns = [(head, one), (head + one, two), (head, one + two)]
        *own_stages, own_both = placed(ring, order[1], columns, pltpu.HBM)
        blocks[0] += around(own, order[2])
        back = moved(own_both, order[2], 3)
        for s, own in enumerate(own_stages, 1):
            ahead = moved(own, order[2], 1)
            blocks[s] += [own, ahead, moved(ahead, order[2], 1), back]

    mixed = []
    for c, order in enumerate(ORDERS):
        taps = conv_taps[:, c * CHANNELS : (c + 1) * CHANNELS]
        mixed.append(mixer(order, tokens, tokens_other, taps, blocks[0][4 * c : 4 * c + 4]))
    own, other = mix_out_product(mixed, blocks[0])
    other = swapped(other)
    first = joined(tokens, own, other, norm_first, False)
    first_other = swapped(first)
    own, other = feed(0, first, first_other, blocks[1])
    other, hidden, down = feed(1, first, first_other, blocks[2], other)
    other = swapped(other)
    own = finished(hidden, down, own)
    return joined(first, own, other, norm_second, True)


def solution(mesh):
    finer = Mesh(
        mesh.devices.reshape(2, 2, 4, 4, 2),
        ("rep", "fs_0", "fs_1", "fs_2", "tp"),
    )
    placement = (
        P(REP_FS_TP, None),
        P(FS, "tp"),
        P(FS, "tp"),
        P(FS, "tp"),
        P(None, "tp"),
        P("tp", FS),
        P(),
        P(FS, "tp"),
        P("tp", FS),
        P(),
    )
    return jax.shard_map(
        local, mesh=finer, in_specs=placement, out_specs=P(REP_FS_TP, None), check_vma=False
    )
```
